256 devices in a mesh: sp: 32 (over z, x), tp: 8 (over y, core).
Axes of the slice: x: 4, y: 4, z: 8, core: 2. Of those that a mesh axis runs over, the one named last changes fastest.
Arguments:
- out_grad: bfloat16 [4096, 2048], P('sp', 'tp'), may hold values from -6 to 6
- moe_input: bfloat16 [4096, 2048], P('sp', 'tp'), may hold values from -6 to 6
- route_weight: float32 [4096, 2], P('sp'), may hold values from 0.2 to 1
- route_ids: int32 [4096, 2], P('sp'), may hold values from 0 to 31, all different within a row; in each aligned block of 128 rows (0 to 127, 128 to 255, ...) at most 16 rows name the same one
- gate_proj: bfloat16 [32, 2048, 2816], P('sp', None, 'tp'), may hold values from -0.125 to 0.125
- up_proj: bfloat16 [32, 2048, 2816], P('sp', None, 'tp'), may hold values from -0.125 to 0.125
- down_proj: bfloat16 [32, 2816, 2048], P('sp', 'tp'), may hold values from -0.109375 to 0.109375
- out_proj: bfloat16 [2048, 2048], P(None, 'tp'), may hold values from -0.125 to 0.125
- conv_out: bfloat16 [4096, 2048], P('sp', 'tp'), may hold values from -6 to 6
- gate_b: bfloat16 [4096, 2048], P('sp', 'tp'), may hold values from -6 to 6
- gate_c: bfloat16 [4096, 2048], P('sp', 'tp'), may hold values from -6 to 6
- value_v: bfloat16 [4096, 2048], P('sp', 'tp'), may hold values from -6 to 6
- conv_taps: float32 [3, 2048], P(None, 'tp'), may hold values from -3 to 3
Outputs:
- grad_gate: bfloat16 [32, 2048, 2816], P('sp', None, 'tp')
- grad_up: bfloat16 [32, 2048, 2816], P('sp', None, 'tp')
- grad_down: bfloat16 [32, 2816, 2048], P('sp', 'tp')
- grad_out: float32 [2048, 2048], P('sp', 'tp')
- grad_b: bfloat16 [4096, 2048], P('sp', 'tp')
- grad_c: bfloat16 [4096, 2048], P('sp', 'tp')
- grad_v: bfloat16 [4096, 2048], P('sp', 'tp')
The draws below stay inside these ranges and needn't reach their ends.
Inputs may be any that keep to these rules, and one draw needn't show every extreme that they name: `route_ids`: each row names two different experts; within the 128 rows of one index of sp no expert is named by more than 16 rows, a bound that some block reaches.
All inputs are finite; a program needn't handle non-finite values.
Results may differ from the reference program's by a relative error of at most 0.019.
Values may be sent and summed in bfloat16 or wider, within the bound.
No kernel may reach another device: no remote copies, remote signals or barrier semaphores. Data moves between devices by JAX's collectives and lax.ppermute only.
A program may use at most 64 MiB of HBM per device.

```python
import math
import jax
import jax.numpy as jnp
import numpy as np
from jax import lax

D = 2048
FF = 2816
TOK_DEV = 128
TOKENS = 4096
EXPERTS = 32
CAP = 16
N_SP = 32
N_TP = 8


def with_spikes(drawn, key, source, target, shards_of, factor):
    owner, partner = [(jnp.arange(drawn.shape[axis_at]) // (drawn.shape[axis_at] // shards_of)).reshape([-1 if axis == axis_at else 1 for axis in range(drawn.ndim)]) for axis_at in (source, target)]
    chosen = jax.random.permutation(key, shards_of)[partner]
    strong = (owner == chosen) | (owner == (partner + shards_of // 2) % shards_of)
    return jnp.where(strong, factor * drawn, drawn)


def block_levels(rng, shape, pieces, smallest, top_value):
    def one(axis_at, blocks):
        heights = jax.random.uniform(jax.random.fold_in(jax.random.fold_in(rng, 6), axis_at), (blocks,), jnp.float32, smallest / len(pieces), top_value / len(pieces))
        return jnp.repeat(jnp.exp(heights), shape[axis_at] // blocks).reshape((-1,) + (1,) * (len(shape) - axis_at - 1))

    level = one(*pieces[0])
    for cut in pieces[1:]:
        level = level * one(*cut)
    return level


def routed_block(key, own, number, rows, amount, top, bound, skew):
    order = jax.random.permutation(key, amount)
    crowded, ordinary = portions_of(amount, rows * top, bound, skew, True), portions_of(amount, rows * top, bound, skew, False)
    places = jnp.arange(amount)

    def named(sizes, rotation):
        used = int((sizes > 0).sum())
        fixed = max(1, used // 4)
        passed = fixed + (places - fixed + rotation * (used - fixed)) % max(1, amount - fixed)
        return jnp.zeros((amount,), jnp.int32).at[order[jnp.where(places < fixed, places, passed)]].set(jnp.asarray(sizes, jnp.int32))

    sizes = jnp.where(number % 4 == 0, named(crowded, number // 4), named(ordinary, number - number // 4 - 1))
    mixed = jax.random.permutation(jax.random.fold_in(own, 3), amount)
    donor, sink = mixed[0:amount // 2 * 2:2], mixed[1:amount // 2 * 2:2]
    room = jnp.minimum(sizes[donor] - 1, bound - sizes[sink]) // 2
    room = jnp.where((donor == order[0]) | (sink == order[0]) | (sizes[sink] == 0), 0, jnp.maximum(room, 0))
    passed = jax.random.randint(jax.random.fold_in(own, 4), (amount // 2,), 0, 1 << 20) % (room + 1)
    sizes = sizes.at[donor].add(-passed).at[sink].add(passed)
    labels = jnp.searchsorted(jnp.cumsum(sizes), jnp.arange(rows * top), side="right").astype(jnp.int32)
    grid = labels.reshape(top, rows).T
    grid = grid[jax.random.permutation(jax.random.fold_in(own, 1), rows)]
    rotation = jax.random.randint(jax.random.fold_in(own, 2), (rows, 1), 0, top)
    return jnp.take_along_axis(grid, (jnp.arange(top)[None, :] + rotation) % top, axis=1)


def portions_of(count, total, most, skew, full):
    weights = [(1 << 20) // math.isqrt(standing ** skew) + 1 for standing in range(1, count + 1)]
    largest = most if full else min(most, max(-(-total // count), total * weights[0] // sum(weights)))
    least = 1 if total - largest >= count - 1 else 0
    given, surplus = [largest] + [least] * (count - 1), total - largest - least * (count - 1)
    while surplus > 0:
        movable = [i for i in range(1, count) if given[i] < largest] or [i for i in range(1, count) if given[i] < most]
        mass, left = sum([weights[i] for i in movable]), surplus
        for i in movable:
            addition = min(most - given[i], max(1, left * weights[i] // mass), surplus)
            given[i] = given[i] + addition
            surplus = surplus - addition
    return np.array(given)


def normal_values(rng, shape, deviation, reach, split=(), kind=jnp.bfloat16):
    loudness = block_levels(rng, shape, split, -0.22, 0.18) if split else 1.0
    values = jax.random.normal(rng, shape, jnp.float32) * deviation * loudness
    return jnp.minimum(jnp.maximum(values, -reach), reach).astype(kind)


def bell_draw_with(rng, extent, spread, limit, pieces, heavy, held_as=jnp.bfloat16):
    array = spread * jax.random.normal(rng, extent, jnp.float32)
    if pieces:
        array = array * block_levels(rng, extent, pieces, -0.22, 0.18)
    return jnp.clip(with_spikes(array, jax.random.fold_in(rng, 3), *heavy), -limit, limit).astype(held_as)


def setup_inputs(seed: int = 0) -> dict:
    arg_keys = jax.random.split(jax.random.key(seed), 14)
    out_grad = bell_draw_with(arg_keys[0], (TOKENS, D), 1.0, 6.0, ((0, 32), (1, 8)), (0, 1, 32, 2.75))
    moe_input = normal_values(arg_keys[1], (TOKENS, D), 1.0, 6.0, ((0, 32), (1, 8)))
    route_weight = jnp.clip(jnp.exp(math.log(1.0) - 1.609438 * jax.random.uniform(arg_keys[2], (TOKENS, 2), jnp.float32) ** block_levels(arg_keys[2], (TOKENS, 2), ((0, 32),), -0.2, 0.2)), 0.2, 1.0)
    route_ids_keys = jax.random.split(jax.random.fold_in(arg_keys[3], 1), TOKENS // TOK_DEV)
    route_ids_turns = jax.random.permutation(jax.random.fold_in(arg_keys[3], 3), TOKENS // TOK_DEV)
    route_ids = jax.vmap(lambda own, number: routed_block(jax.random.fold_in(arg_keys[3], 2), own, number, TOK_DEV, EXPERTS, 2, CAP, 1))(route_ids_keys, route_ids_turns).reshape((TOKENS, 2))
    gate_proj = normal_values(arg_keys[4], (EXPERTS, D, FF), D ** -0.5, 0.125, ((0, 32), (2, 8)))
    up_proj = normal_values(arg_keys[5], (EXPERTS, D, FF), D ** -0.5, 0.125, ((0, 32), (2, 8)))
    down_proj = normal_values(arg_keys[6], (EXPERTS, FF, D), FF ** -0.5, 0.109375, ((0, 32), (1, 8)))
    out_proj = normal_values(arg_keys[7], (D, D), D ** -0.5, 0.125, ((1, 8),))
    conv_out = normal_values(arg_keys[8], (TOKENS, D), 1.0, 6.0, ((0, 32), (1, 8)))
    gate_b = normal_values(arg_keys[9], (TOKENS, D), 1.0, 6.0, ((0, 32), (1, 8)))
    gate_c = normal_values(arg_keys[10], (TOKENS, D), 1.0, 6.0, ((0, 32), (1, 8)))
    value_v = normal_values(arg_keys[11], (TOKENS, D), 1.0, 6.0, ((0, 32), (1, 8)))
    conv_taps = normal_values(arg_keys[12], (3, D), 0.6, 3.0, ((1, 8),), jnp.float32)
    return {"out_grad": out_grad, "moe_input": moe_input, "route_weight": route_weight, "route_ids": route_ids, "gate_proj": gate_proj, "up_proj": up_proj, "down_proj": down_proj, "out_proj": out_proj, "conv_out": conv_out, "gate_b": gate_b, "gate_c": gate_c, "value_v": value_v, "conv_taps": conv_taps}


def slot_table(route_ids):
    flat = route_ids.reshape(N_SP, TOK_DEV * 2).astype(jnp.int32)
    onehot = (flat[:, :, None] == jnp.arange(EXPERTS, dtype=jnp.int32)[None, None, :]).astype(jnp.int32)
    before = jnp.cumsum(onehot, axis=1) - onehot
    slot = jnp.sum(before * onehot, axis=2).astype(jnp.int32)
    return (flat * CAP + slot).astype(jnp.int32)


def place_rows(rows, index):
    return jnp.zeros((EXPERTS * CAP, rows.shape[1]), rows.dtype).at[index].set(rows)


def reference(out_grad, moe_input, route_weight, route_ids, gate_proj, up_proj, down_proj, out_proj, conv_out, gate_b, gate_c, value_v, conv_taps):
    dest = slot_table(route_ids)
    sent = (route_weight[:, :, None] * out_grad.astype(jnp.float32)[:, None, :]).astype(jnp.bfloat16)
    rows_x = jnp.broadcast_to(moe_input[:, None, :], (TOKENS, 2, D)).reshape(N_SP, 2 * TOK_DEV, D)
    rows_dy = sent.reshape(N_SP, 2 * TOK_DEV, D)
    slots_x = jax.vmap(place_rows)(rows_x, dest).reshape(N_SP, EXPERTS, CAP, D)
    slots_dy = jax.vmap(place_rows)(rows_dy, dest).reshape(N_SP, EXPERTS, CAP, D)
    width = FF // N_TP

    def expert(index):
        xin = slots_x[:, index].reshape(N_SP * CAP, D)
        dyin = slots_dy[:, index].reshape(N_SP * CAP, D)
        w_gate = gate_proj[index]
        w_up = up_proj[index]
        w_down = down_proj[index]
        gate = jnp.dot(xin, w_gate, preferred_element_type=jnp.float32)
        upval = jnp.dot(xin, w_up, preferred_element_type=jnp.float32)
        sig = jax.nn.sigmoid(gate)
        act = gate * sig
        hidden = (act * upval).astype(jnp.bfloat16)
        g_down = jnp.dot(hidden.T, dyin, preferred_element_type=jnp.float32).astype(jnp.bfloat16)
        dhid = jnp.dot(dyin, w_down.T, preferred_element_type=jnp.float32)
        dgate = (dhid * upval * (sig * (1.0 + gate * (1.0 - sig)))).astype(jnp.bfloat16)
        dup = (dhid * act).astype(jnp.bfloat16)
        g_gate = jnp.dot(xin.T, dgate, preferred_element_type=jnp.float32).astype(jnp.bfloat16)
        g_up = jnp.dot(xin.T, dup, preferred_element_type=jnp.float32).astype(jnp.bfloat16)
        rows = N_SP * CAP
        part = jnp.einsum('rpf,dpf->prd', dgate.reshape(rows, N_TP, width).astype(jnp.float32),
                          w_gate.reshape(D, N_TP, width).astype(jnp.float32))
        part = part + jnp.einsum('rpf,dpf->prd', dup.reshape(rows, N_TP, width).astype(jnp.float32),
                                 w_up.reshape(D, N_TP, width).astype(jnp.float32))
        part = lax.optimization_barrier(part.astype(jnp.bfloat16)).astype(jnp.float32)
        back = jnp.sum(part, axis=0).astype(jnp.bfloat16)
        return g_gate, g_up, g_down, back

    grad_gate, grad_up, grad_down, backs = lax.map(expert, jnp.arange(EXPERTS, dtype=jnp.int32))
    backs = backs.reshape(EXPERTS, N_SP, CAP, D).transpose(1, 0, 2, 3).reshape(N_SP, EXPERTS * CAP, D)
    picked = jax.vmap(lambda table, index: table[index])(backs, dest)
    moe_grad = jnp.sum(picked.reshape(TOKENS, 2, D).astype(jnp.float32), axis=1)
    grad_h = (out_grad.astype(jnp.float32) + moe_grad).astype(jnp.bfloat16)
    grad_z = jnp.dot(grad_h, out_proj, preferred_element_type=jnp.float32)
    dconv = (grad_z * gate_b.astype(jnp.float32)).astype(jnp.bfloat16)
    grad_b = (grad_z * conv_out.astype(jnp.float32)).astype(jnp.bfloat16)
    padded = jnp.pad(dconv.astype(jnp.float32), ((1, 1), (0, 0)))
    grad_u = conv_taps[0] * padded[2:] + conv_taps[1] * padded[1:-1] + conv_taps[2] * padded[:-2]
    grad_c = (grad_u * value_v.astype(jnp.float32)).astype(jnp.bfloat16)
    grad_v = (grad_u * gate_c.astype(jnp.float32)).astype(jnp.bfloat16)
    mixed = (gate_b.astype(jnp.float32) * conv_out.astype(jnp.float32)).astype(jnp.bfloat16)
    grad_out = jnp.dot(grad_h.T, mixed, preferred_element_type=jnp.float32)
    return grad_gate, grad_up, grad_down, grad_out, grad_b, grad_c, grad_v
```

```python
import jax
import jax.numpy as jnp
from jax import lax
from jax.experimental import pallas as pl
from jax.experimental.pallas import tpu as pltpu
from jax.sharding import Mesh
from jax.sharding import PartitionSpec as P

SP = ("z", "x")
TP = ("y", "c")
BF = jnp.bfloat16
F32 = jnp.float32

VMEM = pl.BlockSpec(memory_space=pltpu.VMEM)
SMEM = pl.BlockSpec(memory_space=pltpu.SMEM)


def call(body, outs, n_smem, args, scratch=(), flops=0, limit=None):
    return pl.pallas_call(
        body,
        out_shape=outs,
        in_specs=[SMEM] * n_smem + [VMEM] * (len(args) - n_smem),
        out_specs=[VMEM] * len(outs),
        scratch_shapes=list(scratch),
        cost_estimate=pl.CostEstimate(flops=flops, bytes_accessed=0, transcendentals=0),
        compiler_params=pltpu.CompilerParams(vmem_limit_bytes=limit),
    )(*args)


def nt(a, b):
    return lax.dot_general(a, b, (((1,), (1,)), ((), ())), preferred_element_type=F32)


def tn(a, b):
    return lax.dot_general(a, b, (((0,), (0,)), ((), ())), preferred_element_type=F32)


def nn(a, b):
    return jnp.dot(a, b, preferred_element_type=F32)


def shift(x, axis, n, k):
    return lax.ppermute(x, axis, [(i, (i + k) % n) for i in range(n)])


def dispatch_kernel(x_ref, og_ref, w_ref, ids_ref, b_ref, co_ref, send_ref, sel_ref, mixed_ref):
    tok = x_ref.shape[0]
    n_exp, cap2, _ = send_ref.shape
    cap = cap2 // 2
    total = n_exp * cap
    up = (
        lax.broadcasted_iota(jnp.int32, (tok, tok), 0)
        < lax.broadcasted_iota(jnp.int32, (tok, tok), 1)
    ).astype(F32).astype(BF)
    expert = lax.broadcasted_iota(jnp.int32, (n_exp, tok), 0)
    rows = []
    for k in range(2):
        wide = jnp.broadcast_to(ids_ref[:, k : k + 1].astype(F32), (tok, tok))
        rows.append(wide.T.astype(jnp.int32))
    hot = [(r[:n_exp] == expert).astype(F32) for r in rows]
    before = nn((hot[0] + hot[1]).astype(BF), up)
    og = og_ref[...].astype(F32)
    slot_iota = lax.broadcasted_iota(jnp.int32, (total, tok), 0)
    lane = lax.broadcasted_iota(jnp.int32, (tok, tok), 1)
    place, sent, cols = [], [], []
    for k in range(2):
        slot = jnp.sum(before * hot[k], axis=0, keepdims=True)
        dest = rows[k][:1].astype(F32) * cap + slot
        cols.append(jnp.broadcast_to(dest, (tok, tok)).T.astype(jnp.int32))
        place.append((slot_iota == dest.astype(jnp.int32)).astype(F32).astype(BF))
        sent.append((w_ref[:, k : k + 1] * og).astype(BF))
    sx = nn(place[0] + place[1], x_ref[...]).astype(BF)
    sy = (nn(place[0], sent[0]) + nn(place[1], sent[1])).astype(BF)
    send_ref[:, :cap, :] = sx.reshape(n_exp, cap, sx.shape[1])
    send_ref[:, cap:, :] = sy.reshape(n_exp, cap, sy.shape[1])
    for j in range(total // tok):
        hit = (cols[0] == lane + j * tok) | (cols[1] == lane + j * tok)
        sel_ref[:, j * tok : (j + 1) * tok] = hit.astype(F32).astype(BF)
    mixed_ref[...] = (b_ref[...].astype(F32) * co_ref[...].astype(F32)).astype(BF)


def expert_kernel(y_ref, c_ref, *refs):
    pieces, (wg_ref, wu_ref, wd_ref) = refs[:16], refs[16:19]
    theirs_ref, mine_ref, x_ref, dy_ref, hid_ref, dg_ref, du_ref, g_s, u_s, h_s = refs[19:]
    y, c = y_ref[0], c_ref[0]
    ch = pieces[0].shape[1]

    def at(d, core):
        return pl.multiple_of(ch * (2 * lax.rem(y + d, 4) + core), ch)

    for d in range(4):
        for other in range(2):
            core = c if other == 0 else 1 - c
            x_ref[:, pl.ds(at(d, core), ch)] = pieces[4 * d + 2 * other][...]
            dy_ref[:, pl.ds(at(d, core), ch)] = pieces[4 * d + 2 * other + 1][...]
    g_s[...] = nn(x_ref[...], wg_ref[...])
    u_s[...] = nn(x_ref[...], wu_ref[...])
    h_s[...] = nt(dy_ref[...], wd_ref[...])
    step = 64
    for r in range(0, g_s.shape[0], step):
        g, u, dh = g_s[r : r + step], u_s[r : r + step], h_s[r : r + step]
        sig = jax.nn.sigmoid(g)
        act = g * sig
        hid_ref[r : r + step] = (act * u).astype(BF)
        dg_ref[r : r + step] = (dh * u * (sig * (1.0 + g * (1.0 - sig)))).astype(BF)
        du_ref[r : r + step] = (dh * act).astype(BF)
    for ref, core in ((theirs_ref, 1 - c), (mine_ref, c)):
        for d in range(4):
            o = at(d, core)
            ref[d] = (
                nt(dg_ref[...], wg_ref[pl.ds(o, ch), :]) + nt(du_ref[...], wu_ref[pl.ds(o, ch), :])
            ).astype(BF)


def combine_kernel(sel_ref, back_ref, og_ref, dh_ref):
    dh_ref[...] = (og_ref[...].astype(F32) + nn(sel_ref[...], back_ref[...])).astype(BF)


def dz_kernel(y_ref, c_ref, own_ref, part_ref, w_ref, b_ref, co_ref, gb_ref, dc_ref, first_ref, last_ref):
    y, c = y_ref[0], c_ref[0]
    tok, ch = b_ref.shape
    acc = jnp.zeros((tok, w_ref.shape[1]), F32)
    for d in range(4):
        for ref, core in ((own_ref, c), (part_ref, 1 - c)):
            o = pl.multiple_of(ch * (2 * lax.rem(y + d, 4) + core), ch)
            acc = acc + nn(ref[d * tok : (d + 1) * tok, :], w_ref[pl.ds(o, ch), :])
    gb_ref[...] = (acc * co_ref[...].astype(F32)).astype(BF)
    dc = (acc * b_ref[...].astype(F32)).astype(BF)
    dc_ref[...] = dc
    first_ref[...] = dc[:1]
    last_ref[...] = dc[tok - 1 :]


def conv_kernel(dc_ref, low_ref, high_ref, t_ref, v_ref, g_ref, gc_ref, gv_ref):
    dc = dc_ref[...].astype(F32)
    tok = dc.shape[0]
    row = lax.broadcasted_iota(jnp.int32, dc.shape, 0)
    nxt = jnp.where(row == tok - 1, high_ref[...].astype(F32), pltpu.roll(dc, tok - 1, 0))
    prv = jnp.where(row == 0, low_ref[...].astype(F32), pltpu.roll(dc, 1, 0))
    du = t_ref[0:1, :] * nxt + t_ref[1:2, :] * dc + t_ref[2:3, :] * prv
    gc_ref[...] = (du * v_ref[...].astype(F32)).astype(BF)
    gv_ref[...] = (du * g_ref[...].astype(F32)).astype(BF)


def outer_kernel(y_ref, c_ref, z_ref, own_ref, part_ref, mix_ref, out_ref, a_s, b_s):
    y, c, z = y_ref[0], c_ref[0], z_ref[0]
    tok = own_ref.shape[0] // 4
    for d in range(4):
        for ref, core in ((own_ref, c), (part_ref, 1 - c)):
            o = pl.multiple_of(tok * (2 * lax.rem(y + d, 4) + core), tok)
            a_s[pl.ds(o, tok), :] = ref[d * tok : (d + 1) * tok, :]
    for d in range(8):
        o = pl.multiple_of(tok * (z ^ d), tok)
        b_s[pl.ds(o, tok), :] = mix_ref[d * tok : (d + 1) * tok, :]
    out_ref[...] = tn(a_s[...], b_s[...]).astype(BF).reshape(out_ref.shape)


def over_tp(x):
    parts = [x] + [shift(x, "y", 4, 4 - k) for k in (1, 2, 3)]
    own = jnp.concatenate(parts, axis=0)
    return own, shift(own, "c", 2, 1)


def local(
    out_grad, moe_input, route_weight, route_ids, gate_proj, up_proj, down_proj,
    out_proj, conv_out, gate_b, gate_c, value_v, conv_taps,
):
    tok, ch = out_grad.shape
    n_exp = lax.axis_size(SP)
    cap = 4 * tok // n_exp
    total = n_exp * cap
    yi = lax.axis_index("y").astype(jnp.int32).reshape(1)
    ci = lax.axis_index("c").astype(jnp.int32).reshape(1)
    zi = lax.axis_index("z").astype(jnp.int32).reshape(1)
    sds = jax.ShapeDtypeStruct
    send, sel, mixed = call(
        dispatch_kernel,
        [sds((n_exp, 2 * cap, ch), BF), sds((tok, total), BF), sds((tok, ch), BF)],
        0,
        (moe_input, out_grad, route_weight, route_ids, gate_b, conv_out),
    )
    recv = lax.all_to_all(send, SP, 0, 0, tiled=True)
    hx = recv[:, :cap].reshape(total, ch)
    hy = recv[:, cap:].reshape(total, ch)
    ax = shift(hx, "y", 4, 1)
    by = shift(hy, "y", 4, 3)
    ay = shift(hy, "y", 4, 1)
    bx = shift(hx, "y", 4, 3)
    fx = shift(ax, "y", 4, 1)
    fy = shift(by, "y", 4, 3)
    mix = mixed
    for bit in (1, 2, 4):
        other = lax.ppermute(mix, "z", [(i, i ^ bit) for i in range(8)])
        mix = jnp.concatenate([mix, other], axis=0)
    pieces = []
    for px, py in ((hx, hy), (bx, by), (fx, fy), (ax, ay)):
        pieces += [px, py, shift(px, "c", 2, 1), shift(py, "c", 2, 1)]
    w_gate, w_up, w_down = gate_proj[0], up_proj[0], down_proj[0]
    d, f = w_gate.shape
    theirs, mine, xin, dyin, hidden, dgate, dup = call(
        expert_kernel,
        [sds((4, total, ch), BF)] * 2 + [sds((total, d), BF)] * 2 + [sds((total, f), BF)] * 3,
        2,
        (yi, ci, *pieces, w_gate, w_up, w_down),
        scratch=[pltpu.VMEM((total, f), F32)] * 3,
        flops=10 * total * d * f,
    )
    got = shift(theirs, "c", 2, 1)
    half = total // 2
    pair = (mine.astype(F32) + got.astype(F32)).astype(BF)
    a0 = shift(pair[2, :half], "y", 4, 1)
    b0 = shift(pair[2, half:], "y", 4, 3)
    a1 = shift(pair[1, half:], "y", 4, 1)
    b1 = shift(pair[3, :half], "y", 4, 3)
    a2 = shift((pair[1, :half].astype(F32) + a0.astype(F32)).astype(BF), "y", 4, 1)
    b2 = shift((pair[3, half:].astype(F32) + b0.astype(F32)).astype(BF), "y", 4, 3)
    lo = pair[0, :half].astype(F32) + a2.astype(F32) + b1.astype(F32)
    hi = pair[0, half:].astype(F32) + a1.astype(F32) + b2.astype(F32)
    summed = jnp.concatenate([lo, hi], axis=0).astype(BF)
    grad_down = tn(hidden, dyin).astype(BF)
    grad_gate = tn(xin, dgate).astype(BF)
    grad_up = tn(xin, dup).astype(BF)
    back = lax.all_to_all(summed.reshape(n_exp, cap, ch), SP, 0, 0, tiled=True)
    (dh,) = call(
        combine_kernel, [sds((tok, ch), BF)], 0, (sel, back.reshape(total, ch), out_grad)
    )
    swap = [((z, y, c), (y * 2 + c, z // 2, z % 2)) for z in range(8) for y in range(4) for c in range(2)]
    turned = lax.ppermute(
        dh, ("z", "y", "c"), [(a[0] * 8 + a[1] * 2 + a[2], b[0] * 8 + b[1] * 2 + b[2]) for a, b in swap]
    )
    h_own, h_part = over_tp(dh)
    t_own, t_part = over_tp(turned)
    grad_b, dconv, first, last = call(
        dz_kernel,
        [sds((tok, ch), BF), sds((tok, ch), BF), sds((1, ch), BF), sds((1, ch), BF)],
        2,
        (yi, ci, h_own, h_part, out_proj, gate_b, conv_out),
        flops=2 * tok * d * ch,
    )
    low = lax.ppermute(last, SP, [(i, i + 1) for i in range(n_exp - 1)])
    high = lax.ppermute(first, SP, [(i + 1, i) for i in range(n_exp - 1)])
    (terms,) = call(
        outer_kernel,
        [sds((4, ch // 4, ch), BF)],
        3,
        (yi, ci, zi, t_own, t_part, mix),
        scratch=[pltpu.VMEM((8 * tok, ch), BF)] * 2,
        flops=16 * tok * ch * ch,
    )
    grad_c, grad_v = call(
        conv_kernel,
        [sds((tok, ch), BF)] * 2,
        0,
        (dconv, low, high, conv_taps, value_v, gate_c),
    )
    grad_out = lax.all_to_all(terms, "x", 0, 0, tiled=True).astype(F32).sum(axis=0)
    return (grad_gate[None], grad_up[None], grad_down[None], grad_out, grad_b, grad_c, grad_v)


def solution(mesh):
    split = Mesh(mesh.devices.reshape(8, 4, 4, 2), ("z", "x", "y", "c"))
    return jax.shard_map(
        local,
        mesh=split,
        in_specs=(
            P(SP, TP), P(SP, TP), P(SP, None), P(SP, None), P(SP, None, TP), P(SP, None, TP),
            P(SP, TP, None), P(None, TP), P(SP, TP), P(SP, TP), P(SP, TP), P(SP, TP), P(None, TP),
        ),
        out_specs=(
            P(SP, None, TP), P(SP, None, TP), P(SP, TP, None), P(SP, TP), P(SP, TP), P(SP, TP), P(SP, TP),
        ),
        check_vma=False,
    )
```

```python
import jax
import jax.numpy as jnp
from jax import lax
from jax.experimental import pallas as pl
from jax.experimental.pallas import tpu as pltpu
from jax.sharding import Mesh
from jax.sharding import PartitionSpec as P

SP = ("z", "x")
TP = ("y", "c")
BF = jnp.bfloat16
F32 = jnp.float32

VMEM = pl.BlockSpec(memory_space=pltpu.VMEM)
SMEM = pl.BlockSpec(memory_space=pltpu.SMEM)
ANY = pl.BlockSpec(memory_space=pltpu.HBM)


def call(body, outs, n_smem, args, scratch=(), flops=0, hbm_outs=(), limit=8, hbm_args=(), any_args=(), kind=BF):
    args = [
        a if i < n_smem else pltpu.with_memory_space_constraint(a, pltpu.HBM if i in hbm_args or i in any_args else pltpu.VMEM)
        for i, a in enumerate(args)
    ]
    outs = [
        jax.ShapeDtypeStruct(shape, kind) if i in hbm_outs else pltpu.VMEM(shape, BF)
        for i, shape in enumerate(outs)
    ]
    return pl.pallas_call(
        body,
        out_shape=outs,
        in_specs=[SMEM if i < n_smem else ANY if i in any_args else VMEM for i in range(len(args))],
        out_specs=[VMEM] * len(outs),
        scratch_shapes=list(scratch),
        cost_estimate=pl.CostEstimate(flops=flops, bytes_accessed=0, transcendentals=0),
        compiler_params=pltpu.CompilerParams(vmem_limit_bytes=limit << 20),
    )(*args)


def nt(a, b):
    return lax.dot_general(a, b, (((1,), (1,)), ((), ())), preferred_element_type=F32)


def tn(a, b):
    return lax.dot_general(a, b, (((0,), (0,)), ((), ())), preferred_element_type=F32)


def nn(a, b):
    return jnp.dot(a, b, preferred_element_type=F32)


def shift(x, axis, n, k):
    return lax.ppermute(x, axis, [(i, (i + k) % n) for i in range(n)])


def dispatch_kernel(x_ref, og_ref, w_ref, ids_ref, send_ref, sel_ref):
    tok, ch = x_ref.shape
    n_exp, cap2, _ = send_ref.shape
    cap = cap2 // 2
    total = n_exp * cap
    up = (
        lax.broadcasted_iota(jnp.int32, (tok, tok), 0)
        < lax.broadcasted_iota(jnp.int32, (tok, tok), 1)
    ).astype(F32).astype(BF)
    expert = lax.broadcasted_iota(jnp.int32, (n_exp, tok), 0)
    ids = [ids_ref[k : k + 1, :] for k in range(2)]
    hot = [(i == expert).astype(F32) for i in ids]
    before = nn((hot[0] + hot[1]).astype(BF), up)
    slot_iota = lax.broadcasted_iota(jnp.int32, (total, tok), 0)
    lane = lax.broadcasted_iota(jnp.int32, (tok, tok), 1)
    place, sent, cols = [], [], []
    for k in range(2):
        slot = jnp.sum(before * hot[k], axis=0, keepdims=True)
        dest = ids[k].astype(F32) * cap + slot
        cols.append(jnp.broadcast_to(dest, (tok, tok)).T.astype(jnp.int32))
        place.append((slot_iota == dest.astype(jnp.int32)).astype(F32).astype(BF))
        weight = jnp.broadcast_to(w_ref[k : k + 1, :], (tok, tok)).T
        sent.append(
            jnp.concatenate(
                [(weight * og_ref[:, j : j + tok].astype(F32)).astype(BF) for j in range(0, ch, tok)], axis=1
            )
        )
    sx = nn(place[0] + place[1], x_ref[...]).astype(BF)
    sy = (nn(place[0], sent[0]) + nn(place[1], sent[1])).astype(BF)
    send_ref[:, :cap, :] = sx.reshape(n_exp, cap, ch)
    send_ref[:, cap:, :] = sy.reshape(n_exp, cap, ch)
    for j in range(total // tok):
        hit = (cols[0] == lane + j * tok) | (cols[1] == lane + j * tok)
        sel_ref[:, j * tok : (j + 1) * tok] = hit.astype(F32).astype(BF)


def mixed_kernel(b_ref, co_ref, mixed_ref):
    mixed_ref[...] = (b_ref[...].astype(F32) * co_ref[...].astype(F32)).astype(BF)


def load_kernel(gate_ref, up_ref, down_ref, w_ref, wd_ref, sems):
    width = wd_ref.shape[0]
    loads = [
        pltpu.make_async_copy(gate_ref, w_ref.at[pl.ds(0, width)], sems.at[0]),
        pltpu.make_async_copy(up_ref, w_ref.at[pl.ds(width, width)], sems.at[1]),
        pltpu.make_async_copy(down_ref, wd_ref, sems.at[2]),
    ]
    for load in loads:
        load.start()
    for load in loads:
        load.wait()


def expert_kernel(y_ref, c_ref, *refs):
    pieces, w_ref, wd_ref = refs[:16], refs[16], refs[17]
    theirs_ref, x_ref, dy_ref, hid_ref, dgu_ref, d_ref, gu_s, h_s = refs[18:]
    y, c = y_ref[0], c_ref[0]
    ch = pieces[0].shape[1]
    f = hid_ref.shape[0]
    for d in range(4):
        for other in range(2):
            o = channels(y, d, c if other == 0 else 1 - c, ch)
            x_ref[:, pl.ds(o, ch)] = pieces[4 * d + 2 * other][...]
            dy_ref[:, pl.ds(o, ch)] = pieces[4 * d + 2 * other + 1][...]
    gu_s[...] = nt(w_ref[...], x_ref[...])
    h_s[...] = nt(wd_ref[...], dy_ref[...])
    step = 32
    for r in range(0, f, step):
        g, u, dh = gu_s[r : r + step], gu_s[f + r : f + r + step], h_s[r : r + step]
        sig = jax.nn.sigmoid(g)
        act = g * sig
        hid_ref[r : r + step] = (act * u).astype(BF)
        dgu_ref[r : r + step] = (dh * u * (sig * (1.0 + g * (1.0 - sig)))).astype(BF)
        dgu_ref[f + r : f + r + step] = (dh * act).astype(BF)
    d_ref[...] = dgu_ref[...].T
    for d in range(4):
        o = channels(y, d, 1 - c, ch)
        theirs_ref[d] = nn(d_ref[...], w_ref[:, pl.ds(o, ch)]).astype(BF)


def channels(y, d, core, ch):
    return pl.multiple_of(ch * (2 * lax.rem(y + d, 4) + core), ch)


def own_half_kernel(y_ref, c_ref, d_ref, w_ref, mine_ref):
    y, c = y_ref[0], c_ref[0]
    ch = mine_ref.shape[2]
    for d in range(4):
        o = channels(y, d, c, ch)
        mine_ref[d] = nn(d_ref[...], w_ref[:, pl.ds(o, ch)]).astype(BF)


def pair_kernel(mine_ref, got_ref, *out_refs):
    for d in range(4):
        out_refs[d][...] = (mine_ref[d].astype(F32) + got_ref[d].astype(F32)).astype(BF)


def sum_kernel(*refs):
    total = refs[0][...].astype(F32)
    for ref in refs[1:-1]:
        total = total + ref[...].astype(F32)
    refs[-1][...] = total.astype(refs[-1].dtype)


def weights_kernel(x_ref, dy_ref, hid_ref, dgu_ref, gg_ref, gu_ref, gd_ref):
    f = hid_ref.shape[0]
    gg_ref[...] = nn(dgu_ref[:f], x_ref[...]).astype(BF)
    gu_ref[...] = nn(dgu_ref[f:], x_ref[...]).astype(BF)
    gd_ref[...] = nn(hid_ref[...], dy_ref[...]).astype(BF)


def combine_kernel(sel_ref, back_ref, og_ref, b_ref, dh_ref, first_ref, last_ref):
    dh = (og_ref[...].astype(F32) + nn(sel_ref[...], back_ref[...])).astype(BF)
    dh_ref[...] = dh
    tok = dh.shape[0]
    first_ref[0:1] = dh[:1]
    first_ref[1:2] = b_ref[0:1]
    last_ref[0:1] = dh[tok - 1 :]
    last_ref[1:2] = b_ref[tok - 1 :]


def stack_kernel(turned_ref, low_ref, high_ref, out_ref):
    tok, ch = turned_ref.shape
    out_ref[:tok] = turned_ref[...]
    row = lax.broadcasted_iota(jnp.int32, (16, ch), 0)
    low, high = low_ref[0:1].astype(F32), high_ref[0:1].astype(F32)
    out_ref[tok:] = jnp.where(row == 0, low, jnp.where(row == 1, high, 0.0)).astype(BF)


def mixer_kernel(
    y_ref, c_ref, own_ref, part_ref, edge_own_ref, edge_part_ref, w_ref, b_ref, co_ref, bl_ref, bh_ref, t_ref, v_ref, g_ref,
    gb_ref, gc_ref, gv_ref,
):
    y, c = y_ref[0], c_ref[0]
    tok, ch = b_ref.shape
    size = edge_own_ref.shape[0] // 4
    acc = jnp.zeros((size, ch), F32)
    for d in range(4):
        for ref, edge, core in ((own_ref, edge_own_ref, c), (part_ref, edge_part_ref, 1 - c)):
            rows = jnp.concatenate([ref[d * tok : (d + 1) * tok], edge[d * size + tok : (d + 1) * size]], axis=0)
            acc = acc + nn(rows, w_ref[pl.ds(channels(y, d, core, ch), ch), :])
    gb_ref[...] = (acc[:tok] * co_ref[...].astype(F32)).astype(BF)
    dc = (acc[:tok] * b_ref[...].astype(F32)).astype(BF).astype(F32)
    low = (acc[tok : tok + 1] * bl_ref[1:2].astype(F32)).astype(BF).astype(F32)
    high = (acc[tok + 1 : tok + 2] * bh_ref[1:2].astype(F32)).astype(BF).astype(F32)
    row = lax.broadcasted_iota(jnp.int32, dc.shape, 0)
    nxt = jnp.where(row == tok - 1, high, pltpu.roll(dc, tok - 1, 0))
    prv = jnp.where(row == 0, low, pltpu.roll(dc, 1, 0))
    du = t_ref[0:1, :] * nxt + t_ref[1:2, :] * dc + t_ref[2:3, :] * prv
    gc_ref[...] = (du * v_ref[...].astype(F32)).astype(BF)
    gv_ref[...] = (du * g_ref[...].astype(F32)).astype(BF)


def outer_kernel(y_ref, c_ref, z_ref, xi_ref, own_ref, part_ref, mix_ref, *refs):
    out_refs, (a_s, b_s, o_s) = refs[:4], refs[4:]
    y, c, z = y_ref[0], c_ref[0], z_ref[0]
    tok = mix_ref.shape[0] // 8
    size = own_ref.shape[0] // 4
    for d in range(4):
        for ref, core in ((own_ref, c), (part_ref, 1 - c)):
            a_s[pl.ds(channels(y, d, core, tok), tok), :] = ref[d * size : d * size + tok, :]
    for d, bits in enumerate((0, 4, 2, 6, 1, 5, 3, 7)):
        o = pl.multiple_of(tok * (z ^ bits), tok)
        b_s[pl.ds(o, tok), :] = mix_ref[d * tok : (d + 1) * tok, :]
    o_s[...] = tn(a_s[...], b_s[...])
    rows = out_refs[0].shape[0]
    for k, ref in enumerate(out_refs):
        ref[...] = o_s[pl.ds(pl.multiple_of(rows * lax.rem(xi_ref[0] + k, 4), rows), rows), :].astype(BF)


def over_tp(x):
    parts = [x] + [shift(x, "y", 4, 4 - k) for k in (1, 2, 3)]
    own = jnp.concatenate(parts, axis=0)
    return own, shift(own, "c", 2, 1)


def edges(first, last):
    n = lax.axis_size(SP)
    low = lax.ppermute(last, SP, [(i, i + 1) for i in range(n - 1)])
    high = lax.ppermute(first, SP, [(i + 1, i) for i in range(n - 1)])
    return low, high


def widen(x, bit):
    return jnp.concatenate([x, lax.ppermute(x, "z", [(i, i ^ bit) for i in range(8)])], axis=0)


def local(
    out_grad, moe_input, route_weight, route_ids, gate_proj, up_proj, down_proj,
    out_proj, conv_out, gate_b, gate_c, value_v, conv_taps,
):
    tok, ch = out_grad.shape
    n_exp = lax.axis_size(SP)
    cap = 4 * tok // n_exp
    total = n_exp * cap
    yi = lax.axis_index("y").astype(jnp.int32).reshape(1)
    ci = lax.axis_index("c").astype(jnp.int32).reshape(1)
    zi = lax.axis_index("z").astype(jnp.int32).reshape(1)
    xi = lax.axis_index("x").astype(jnp.int32).reshape(1)
    yi, ci, zi, xi, moe_input = lax.optimization_barrier((yi, ci, zi, xi, moe_input))
    send, sel = call(
        dispatch_kernel,
        [(n_exp, 2 * cap, ch), (tok, total)],
        0,
        (moe_input, out_grad, route_weight.T, route_ids.T),
        hbm_args=(0, 1, 2, 3),
    )
    recv = lax.all_to_all(send, SP, 0, 0, tiled=True)
    recv, gate_b, conv_out, gate_proj, up_proj, down_proj = lax.optimization_barrier(
        (recv, gate_b, conv_out, gate_proj, up_proj, down_proj)
    )
    (mixed,) = call(mixed_kernel, [(tok, ch)], 0, (gate_b, conv_out), hbm_args=(0, 1))
    hx = recv[:, :cap].reshape(total, ch)
    hy = recv[:, cap:].reshape(total, ch)
    ax = shift(hx, "y", 4, 1)
    by = shift(hy, "y", 4, 3)
    ay = shift(hy, "y", 4, 1)
    bx = shift(hx, "y", 4, 3)
    mix = widen(mixed, 4)
    f, d = down_proj.shape[1:]
    w_pair, w_down = call(
        load_kernel,
        [(2 * f, d), (f, d)],
        0,
        (gate_proj[0].T, up_proj[0].T, down_proj[0]),
        scratch=[pltpu.SemaphoreType.DMA((3,))],
        any_args=(0, 1, 2),
    )
    ax, by, w_pair, w_down = lax.optimization_barrier((ax, by, w_pair, w_down))
    fx = shift(ax, "y", 4, 1)
    fy = shift(by, "y", 4, 3)
    mix = widen(mix, 2)
    pieces = []
    for px, py in ((hx, hy), (bx, by), (fx, fy), (ax, ay)):
        pieces += [px, py, shift(px, "c", 2, 1), shift(py, "c", 2, 1)]
    mix = widen(mix, 1)
    theirs, xin, dyin, hidden, dgu, dgu_rows = call(
        expert_kernel,
        [(4, total, ch), (total, d), (total, d), (f, total), (2 * f, total), (total, 2 * f)],
        2,
        (yi, ci, *pieces, w_pair, w_down),
        scratch=[pltpu.VMEM((2 * f, total), F32), pltpu.VMEM((f, total), F32)],
        flops=8 * total * d * f,
        limit=24,
    )
    got = shift(theirs, "c", 2, 1)
    (mine,) = call(own_half_kernel, [(4, total, ch)], 2, (yi, ci, dgu_rows, w_pair), flops=2 * total * d * f)
    pair = call(pair_kernel, [(total, ch)] * 4, 0, (mine, got))
    parts = [shift(pair[k], "y", 4, k) for k in (1, 3, 2)]
    gate_t, up_t, grad_down = call(
        weights_kernel,
        [(f, d)] * 3,
        0,
        (xin, dyin, hidden, dgu),
        flops=6 * total * d * f,
        hbm_outs=(0, 1, 2),
        limit=24,
    )
    parts, mix, gate_t, up_t, grad_down = lax.optimization_barrier((parts, mix, gate_t, up_t, grad_down))
    (summed,) = call(sum_kernel, [(total, ch)], 0, (pair[0], *parts))
    back = lax.all_to_all(summed.reshape(n_exp, cap, ch), SP, 0, 0, tiled=True)
    dh, first, last = call(
        combine_kernel, [(tok, ch), (2, ch), (2, ch)], 0, (sel, back.reshape(total, ch), out_grad, gate_b)
    )
    swap = [(z * 8 + y * 2 + c, (y * 2 + c) * 8 + z) for z in range(8) for y in range(4) for c in range(2)]
    turned = lax.ppermute(dh, ("z", "y", "c"), swap)
    low, high = edges(first, last)
    h_own, h_part = over_tp(dh)
    (stack,) = call(stack_kernel, [(tok + 16, ch)], 0, (turned, low, high))
    t_own, t_part = over_tp(stack)
    terms = call(
        outer_kernel,
        [(ch // 4, ch)] * 4,
        4,
        (yi, ci, zi, xi, t_own, t_part, mix),
        scratch=[pltpu.VMEM((8 * tok, ch), BF)] * 2 + [pltpu.VMEM((ch, ch), F32)],
        flops=16 * tok * ch * ch,
    )
    came = [shift(terms[k], "x", 4, k) for k in (1, 3, 2)]
    grad_b, grad_c, grad_v = call(
        mixer_kernel,
        [(tok, ch)] * 3,
        2,
        (yi, ci, h_own, h_part, t_own, t_part, out_proj, gate_b, conv_out, low, high, conv_taps, value_v, gate_c),
        flops=2 * tok * d * ch,
        hbm_outs=(0, 1, 2),
    )
    (grad_out,) = call(sum_kernel, [(ch // 4, ch)], 0, (terms[0], *came), hbm_outs=(0,), kind=F32)
    return (gate_t.T[None], up_t.T[None], grad_down[None], grad_out, grad_b, grad_c, grad_v)


def solution(mesh):
    split = Mesh(mesh.devices.reshape(8, 4, 4, 2), ("z", "x", "y", "c"))
    return jax.shard_map(
        local,
        mesh=split,
        in_specs=(
            P(SP, TP), P(SP, TP), P(SP, None), P(SP, None), P(SP, None, TP), P(SP, None, TP),
            P(SP, TP, None), P(None, TP), P(SP, TP), P(SP, TP), P(SP, TP), P(SP, TP), P(None, TP),
        ),
        out_specs=(
            P(SP, None, TP), P(SP, None, TP), P(SP, TP, None), P(SP, TP), P(SP, TP), P(SP, TP), P(SP, TP),
        ),
        check_vma=False,
    )
```

```python
import jax
import jax.numpy as jnp
from jax import lax
from jax.experimental import pallas as pl
from jax.experimental.pallas import tpu as pltpu
from jax.sharding import Mesh
from jax.sharding import PartitionSpec as P

SP = ("z", "x")
TP = ("y", "c")
BF = jnp.bfloat16
F32 = jnp.float32

VMEM = pl.BlockSpec(memory_space=pltpu.VMEM)
SMEM = pl.BlockSpec(memory_space=pltpu.SMEM)
ANY = pl.BlockSpec(memory_space=pltpu.HBM)


def call(body, outs, n_smem, args, scratch=(), flops=0, hbm_outs=(), limit=8, hbm_args=(), any_args=(), kind=BF):
    args = [
        a if i < n_smem else pltpu.with_memory_space_constraint(a, pltpu.HBM if i in hbm_args or i in any_args else pltpu.VMEM)
        for i, a in enumerate(args)
    ]
    outs = [
        jax.ShapeDtypeStruct(shape, kind) if i in hbm_outs else pltpu.VMEM(shape, BF)
        for i, shape in enumerate(outs)
    ]
    return pl.pallas_call(
        body,
        out_shape=outs,
        in_specs=[SMEM if i < n_smem else ANY if i in any_args else VMEM for i in range(len(args))],
        out_specs=[VMEM] * len(outs),
        scratch_shapes=list(scratch),
        cost_estimate=pl.CostEstimate(flops=flops, bytes_accessed=0, transcendentals=0),
        compiler_params=pltpu.CompilerParams(vmem_limit_bytes=limit << 20),
    )(*args)


def nt(a, b):
    return lax.dot_general(a, b, (((1,), (1,)), ((), ())), preferred_element_type=F32)


def tn(a, b):
    return lax.dot_general(a, b, (((0,), (0,)), ((), ())), preferred_element_type=F32)


def nn(a, b):
    return jnp.dot(a, b, preferred_element_type=F32)


def shift(x, axis, n, k):
    return lax.ppermute(x, axis, [(i, i ^ k) for i in range(n)])


def dispatch_kernel(x_ref, og_ref, w_ref, ids_ref, send_ref, sel_ref):
    tok, ch = x_ref.shape
    n_exp, cap2, _ = send_ref.shape
    cap = cap2 // 2
    total = n_exp * cap
    up = (
        lax.broadcasted_iota(jnp.int32, (tok, tok), 0)
        < lax.broadcasted_iota(jnp.int32, (tok, tok), 1)
    ).astype(F32).astype(BF)
    expert = lax.broadcasted_iota(jnp.int32, (n_exp, tok), 0)
    ids = [ids_ref[k : k + 1, :] for k in range(2)]
    hot = [(i == expert).astype(F32) for i in ids]
    before = nn((hot[0] + hot[1]).astype(BF), up)
    slot_iota = lax.broadcasted_iota(jnp.int32, (total, tok), 0)
    lane = lax.broadcasted_iota(jnp.int32, (tok, tok), 1)
    place, sent, cols = [], [], []
    for k in range(2):
        slot = jnp.sum(before * hot[k], axis=0, keepdims=True)
        dest = ids[k].astype(F32) * cap + slot
        cols.append(jnp.broadcast_to(dest, (tok, tok)).T.astype(jnp.int32))
        place.append((slot_iota == dest.astype(jnp.int32)).astype(F32).astype(BF))
        weight = jnp.broadcast_to(w_ref[k : k + 1, :], (tok, tok)).T
        sent.append(
            jnp.concatenate(
                [(weight * og_ref[:, j : j + tok].astype(F32)).astype(BF) for j in range(0, ch, tok)], axis=1
            )
        )
    sx = nn(place[0] + place[1], x_ref[...]).astype(BF)
    sy = (nn(place[0], sent[0]) + nn(place[1], sent[1])).astype(BF)
    send_ref[:, :cap, :] = sx.reshape(n_exp, cap, ch)
    send_ref[:, cap:, :] = sy.reshape(n_exp, cap, ch)
    for j in range(total // tok):
        hit = (cols[0] == lane + j * tok) | (cols[1] == lane + j * tok)
        sel_ref[:, j * tok : (j + 1) * tok] = hit.astype(F32).astype(BF)


def mixed_kernel(b_ref, co_ref, mixed_ref):
    mixed_ref[...] = (b_ref[...].astype(F32) * co_ref[...].astype(F32)).astype(BF)


def load_kernel(gate_ref, up_ref, down_ref, w_ref, wd_ref, sems):
    width = wd_ref.shape[0]
    loads = [
        pltpu.make_async_copy(gate_ref, w_ref.at[pl.ds(0, width)], sems.at[0]),
        pltpu.make_async_copy(up_ref, w_ref.at[pl.ds(width, width)], sems.at[1]),
        pltpu.make_async_copy(down_ref, wd_ref, sems.at[2]),
    ]
    for load in loads:
        load.start()
    for load in loads:
        load.wait()


def expert_kernel(y_ref, c_ref, *refs):
    pieces, w_ref, wd_ref = refs[:16], refs[16], refs[17]
    theirs_ref, x_ref, dy_ref, hid_ref, dgu_ref, d_ref, gu_s, h_s = refs[18:]
    y, c = y_ref[0], c_ref[0]
    ch = pieces[0].shape[1]
    f = hid_ref.shape[0]
    for d in range(4):
        for other in range(2):
            o = channels(y, d, c if other == 0 else 1 - c, ch)
            x_ref[:, pl.ds(o, ch)] = pieces[4 * d + 2 * other][...]
            dy_ref[:, pl.ds(o, ch)] = pieces[4 * d + 2 * other + 1][...]
    gu_s[...] = nt(w_ref[...], x_ref[...])
    h_s[...] = nt(wd_ref[...], dy_ref[...])
    step = 32
    for r in range(0, f, step):
        g, u, dh = gu_s[r : r + step], gu_s[f + r : f + r + step], h_s[r : r + step]
        sig = jax.nn.sigmoid(g)
        act = g * sig
        hid_ref[r : r + step] = (act * u).astype(BF)
        dgu_ref[r : r + step] = (dh * u * (sig * (1.0 + g * (1.0 - sig)))).astype(BF)
        dgu_ref[f + r : f + r + step] = (dh * act).astype(BF)
    d_ref[...] = dgu_ref[...].T
    for d in range(4):
        o = channels(y, d, 1 - c, ch)
        theirs_ref[d] = nn(d_ref[...], w_ref[:, pl.ds(o, ch)]).astype(BF)


def channels(y, d, core, ch):
    return pl.multiple_of(ch * (2 * (y ^ d) + core), ch)


def own_half_kernel(y_ref, c_ref, d_ref, w_ref, mine_ref):
    y, c = y_ref[0], c_ref[0]
    ch = mine_ref.shape[2]
    for d in range(4):
        o = channels(y, d, c, ch)
        mine_ref[d] = nn(d_ref[...], w_ref[:, pl.ds(o, ch)]).astype(BF)


def pair_kernel(mine_ref, got_ref, *out_refs):
    for d in range(4):
        out_refs[d][...] = (mine_ref[d].astype(F32) + got_ref[d].astype(F32)).astype(BF)


def sum_kernel(*refs):
    total = refs[0][...].astype(F32)
    for ref in refs[1:-1]:
        total = total + ref[...].astype(F32)
    refs[-1][...] = total.astype(refs[-1].dtype)


def weights_kernel(x_ref, dy_ref, hid_ref, dgu_ref, gg_ref, gu_ref, gd_ref):
    f = hid_ref.shape[0]
    gg_ref[...] = nn(dgu_ref[:f], x_ref[...]).astype(BF)
    gu_ref[...] = nn(dgu_ref[f:], x_ref[...]).astype(BF)
    gd_ref[...] = nn(hid_ref[...], dy_ref[...]).astype(BF)


def combine_kernel(xi_ref, sel_ref, back_ref, og_ref, b_ref, dh_ref, one_ref, two_ref):
    dh = (og_ref[...].astype(F32) + nn(sel_ref[...], back_ref[...])).astype(BF)
    dh_ref[...] = dh
    tok = dh.shape[0]
    even = xi_ref[0] % 2 == 0
    for k, source in enumerate((dh_ref, b_ref)):
        first, last = source[0:1].astype(F32), source[tok - 1 :].astype(F32)
        one_ref[k : k + 1] = jnp.where(even, last, first).astype(BF)
        two_ref[k : k + 1] = jnp.where(even, first, last).astype(BF)


def stack_kernel(turned_ref, dh_ref, low_ref, high_ref, out_ref):
    tok, ch = turned_ref.shape
    out_ref[:tok] = turned_ref[...]
    out_ref[tok : 2 * tok] = dh_ref[...]
    row = lax.broadcasted_iota(jnp.int32, (16, ch), 0)
    low, high = low_ref[0:1].astype(F32), high_ref[0:1].astype(F32)
    out_ref[2 * tok :] = jnp.where(row == 0, low, jnp.where(row == 1, high, 0.0)).astype(BF)


def mixer_kernel(
    y_ref, c_ref, xi_ref, own_ref, part_ref, w_ref, b_ref, co_ref, bl_ref, bh_ref, t_ref, v_ref, g_ref,
    gb_ref, gc_ref, gv_ref,
):
    y, c = y_ref[0], c_ref[0]
    tok, ch = b_ref.shape
    size = own_ref.shape[0] // 4
    acc = jnp.zeros((size - tok, ch), F32)
    for d in range(4):
        for ref, core in ((own_ref, c), (part_ref, 1 - c)):
            acc = acc + nn(ref[d * size + tok : (d + 1) * size, :], w_ref[pl.ds(channels(y, d, core, ch), ch), :])
    gb_ref[...] = (acc[:tok] * co_ref[...].astype(F32)).astype(BF)
    dc = (acc[:tok] * b_ref[...].astype(F32)).astype(BF).astype(F32)
    one = (acc[tok : tok + 1] * bl_ref[1:2].astype(F32)).astype(BF).astype(F32)
    two = (acc[tok + 1 : tok + 2] * bh_ref[1:2].astype(F32)).astype(BF).astype(F32)
    even = xi_ref[0] % 2 == 0
    low, high = jnp.where(even, two, one), jnp.where(even, one, two)
    row = lax.broadcasted_iota(jnp.int32, dc.shape, 0)
    nxt = jnp.where(row == tok - 1, high, pltpu.roll(dc, tok - 1, 0))
    prv = jnp.where(row == 0, low, pltpu.roll(dc, 1, 0))
    du = t_ref[0:1, :] * nxt + t_ref[1:2, :] * dc + t_ref[2:3, :] * prv
    gc_ref[...] = (du * v_ref[...].astype(F32)).astype(BF)
    gv_ref[...] = (du * g_ref[...].astype(F32)).astype(BF)


def outer_kernel(y_ref, c_ref, z_ref, xi_ref, own_ref, part_ref, mix_ref, *refs):
    out_refs, (a_s, b_s, o_s) = refs[:4], refs[4:]
    y, c, z = y_ref[0], c_ref[0], z_ref[0]
    tok = mix_ref.shape[0] // 8
    size = own_ref.shape[0] // 4
    for d in range(4):
        for ref, core in ((own_ref, c), (part_ref, 1 - c)):
            a_s[pl.ds(channels(y, d, core, tok), tok), :] = ref[d * size : d * size + tok, :]
    for d, bits in enumerate((0, 4, 2, 6, 1, 5, 3, 7)):
        o = pl.multiple_of(tok * (z ^ bits), tok)
        b_s[pl.ds(o, tok), :] = mix_ref[d * tok : (d + 1) * tok, :]
    o_s[...] = tn(a_s[...], b_s[...])
    rows = out_refs[0].shape[0]
    for k, ref in enumerate(out_refs):
        ref[...] = o_s[pl.ds(pl.multiple_of(rows * (xi_ref[0] ^ k), rows), rows), :].astype(BF)


def over_tp(x):
    parts = [x] + [shift(x, "y", 4, k) for k in (1, 2, 3)]
    own = jnp.concatenate(parts, axis=0)
    return own, shift(own, "c", 2, 1)


def edges(one, two):
    n = lax.axis_size(SP)
    one = lax.ppermute(one, SP, [(i, i ^ 1) for i in range(n)])
    two = lax.ppermute(two, SP, [(i, i + 1 if i % 2 else i - 1) for i in range(1, n - 1)])
    return one, two


def widen(x, bit):
    return jnp.concatenate([x, lax.ppermute(x, "z", [(i, i ^ bit) for i in range(8)])], axis=0)


def local(
    out_grad, moe_input, route_weight, route_ids, gate_proj, up_proj, down_proj,
    out_proj, conv_out, gate_b, gate_c, value_v, conv_taps,
):
    tok, ch = out_grad.shape
    n_exp = lax.axis_size(SP)
    cap = 4 * tok // n_exp
    total = n_exp * cap
    yi = lax.axis_index("y").astype(jnp.int32).reshape(1)
    ci = lax.axis_index("c").astype(jnp.int32).reshape(1)
    zi = lax.axis_index("z").astype(jnp.int32).reshape(1)
    xi = lax.axis_index("x").astype(jnp.int32).reshape(1)
    yi, ci, zi, xi, moe_input = lax.optimization_barrier((yi, ci, zi, xi, moe_input))
    send, sel = call(
        dispatch_kernel,
        [(n_exp, 2 * cap, ch), (tok, total)],
        0,
        (moe_input, out_grad, route_weight.T, route_ids.T),
        hbm_args=(0, 1, 2, 3),
    )
    recv = lax.all_to_all(send, SP, 0, 0, tiled=True)
    recv, gate_b, conv_out, gate_proj, up_proj, down_proj = lax.optimization_barrier(
        (recv, gate_b, conv_out, gate_proj, up_proj, down_proj)
    )
    (mixed,) = call(mixed_kernel, [(tok, ch)], 0, (gate_b, conv_out), hbm_args=(0, 1))
    hx = recv[:, :cap].reshape(total, ch)
    hy = recv[:, cap:].reshape(total, ch)
    ax = shift(hx, "y", 4, 1)
    by = shift(hy, "y", 4, 3)
    ay = shift(hy, "y", 4, 1)
    bx = shift(hx, "y", 4, 3)
    mix = widen(mixed, 4)
    f, d = down_proj.shape[1:]
    w_pair, w_down = call(
        load_kernel,
        [(2 * f, d), (f, d)],
        0,
        (gate_proj[0].T, up_proj[0].T, down_proj[0]),
        scratch=[pltpu.SemaphoreType.DMA((3,))],
        any_args=(0, 1, 2),
    )
    bx, ay, w_pair, w_down = lax.optimization_barrier((bx, ay, w_pair, w_down))
    fx = shift(bx, "y", 4, 1)
    fy = shift(ay, "y", 4, 3)
    mix = widen(mix, 2)
    pieces = []
    for px, py in ((hx, hy), (ax, ay), (fx, fy), (bx, by)):
        pieces += [px, py, shift(px, "c", 2, 1), shift(py, "c", 2, 1)]
    mix = widen(mix, 1)
    theirs, xin, dyin, hidden, dgu, dgu_rows = call(
        expert_kernel,
        [(4, total, ch), (total, d), (total, d), (f, total), (2 * f, total), (total, 2 * f)],
        2,
        (yi, ci, *pieces, w_pair, w_down),
        scratch=[pltpu.VMEM((2 * f, total), F32), pltpu.VMEM((f, total), F32)],
        flops=8 * total * d * f,
        limit=24,
    )
    got = shift(theirs, "c", 2, 1)
    (mine,) = call(own_half_kernel, [(4, total, ch)], 2, (yi, ci, dgu_rows, w_pair), flops=2 * total * d * f)
    pair = call(pair_kernel, [(total, ch)] * 4, 0, (mine, got))
    parts = [shift(pair[k], "y", 4, k) for k in (1, 3, 2)]
    gate_t, up_t, grad_down = call(
        weights_kernel,
        [(f, d)] * 3,
        0,
        (xin, dyin, hidden, dgu),
        flops=6 * total * d * f,
        hbm_outs=(0, 1, 2),
        limit=24,
    )
    parts, mix, gate_t, up_t, grad_down = lax.optimization_barrier((parts, mix, gate_t, up_t, grad_down))
    (summed,) = call(sum_kernel, [(total, ch)], 0, (pair[0], *parts))
    back = lax.all_to_all(summed.reshape(n_exp, cap, ch), SP, 0, 0, tiled=True)
    dh, one, two = call(
        combine_kernel, [(tok, ch), (2, ch), (2, ch)], 1, (xi, sel, back.reshape(total, ch), out_grad, gate_b)
    )
    swap = [(z * 8 + y * 2 + c, (y * 2 + c) * 8 + z) for z in range(8) for y in range(4) for c in range(2)]
    turned = lax.ppermute(dh, ("z", "y", "c"), swap)
    one, two = edges(one, two)
    (stack,) = call(stack_kernel, [(2 * tok + 16, ch)], 0, (turned, dh, one, two))
    own, part = over_tp(stack)
    terms = call(
        outer_kernel,
        [(ch // 4, ch)] * 4,
        4,
        (yi, ci, zi, xi, own, part, mix),
        scratch=[pltpu.VMEM((8 * tok, ch), BF)] * 2 + [pltpu.VMEM((ch, ch), F32)],
        flops=16 * tok * ch * ch,
    )
    came = [shift(terms[k], "x", 4, k) for k in (1, 3, 2)]
    grad_b, grad_c, grad_v = call(
        mixer_kernel,
        [(tok, ch)] * 3,
        3,
        (yi, ci, xi, own, part, out_proj, gate_b, conv_out, one, two, conv_taps, value_v, gate_c),
        flops=2 * tok * d * ch,
        hbm_outs=(0, 1, 2),
    )
    (grad_out,) = call(sum_kernel, [(ch // 4, ch)], 0, (terms[0], *came), hbm_outs=(0,), kind=F32)
    return (gate_t.T[None], up_t.T[None], grad_down[None], grad_out, grad_b, grad_c, grad_v)


def solution(mesh):
    split = Mesh(mesh.devices.reshape(8, 4, 4, 2), ("z", "x", "y", "c"))
    return jax.shard_map(
        local,
        mesh=split,
        in_specs=(
            P(SP, TP), P(SP, TP), P(SP, None), P(SP, None), P(SP, None, TP), P(SP, None, TP),
            P(SP, TP, None), P(None, TP), P(SP, TP), P(SP, TP), P(SP, TP), P(SP, TP), P(None, TP),
        ),
        out_specs=(
            P(SP, None, TP), P(SP, None, TP), P(SP, TP, None), P(SP, TP), P(SP, TP), P(SP, TP), P(SP, TP),
        ),
        check_vma=False,
    )
```

```python
import jax
import jax.numpy as jnp
from jax import lax
from jax.experimental import pallas as pl
from jax.experimental.pallas import tpu as pltpu
from jax.sharding import Mesh
from jax.sharding import PartitionSpec as P

SP = ("z", "x")
TP = ("y", "c")
BF = jnp.bfloat16
F32 = jnp.float32

VMEM = pl.BlockSpec(memory_space=pltpu.VMEM)
SMEM = pl.BlockSpec(memory_space=pltpu.SMEM)
ANY = pl.BlockSpec(memory_space=pltpu.HBM)


def call(body, outs, n_smem, args, scratch=(), flops=0, hbm_outs=(), limit=8, hbm_args=(), any_args=(), kind=BF):
    args = [
        a if i < n_smem else pltpu.with_memory_space_constraint(a, pltpu.HBM if i in hbm_args or i in any_args else pltpu.VMEM)
        for i, a in enumerate(args)
    ]
    outs = [
        jax.ShapeDtypeStruct(shape, kind) if i in hbm_outs else pltpu.VMEM(shape, BF)
        for i, shape in enumerate(outs)
    ]
    return pl.pallas_call(
        body,
        out_shape=outs,
        in_specs=[SMEM if i < n_smem else ANY if i in any_args else VMEM for i in range(len(args))],
        out_specs=[VMEM] * len(outs),
        scratch_shapes=list(scratch),
        cost_estimate=pl.CostEstimate(flops=flops, bytes_accessed=0, transcendentals=0),
        compiler_params=pltpu.CompilerParams(vmem_limit_bytes=limit << 20),
    )(*args)


def nt(a, b):
    return lax.dot_general(a, b, (((1,), (1,)), ((), ())), preferred_element_type=F32)


def tn(a, b):
    return lax.dot_general(a, b, (((0,), (0,)), ((), ())), preferred_element_type=F32)


def nn(a, b):
    return jnp.dot(a, b, preferred_element_type=F32)


def shift(x, axis, n, k):
    return lax.ppermute(x, axis, [(i, i ^ k) for i in range(n)])


def dispatch_kernel(x_ref, og_ref, w_ref, ids_ref, send_ref, sel_ref):
    tok, ch = x_ref.shape
    n_exp, cap2, _ = send_ref.shape
    cap = cap2 // 2
    total = n_exp * cap
    up = (
        lax.broadcasted_iota(jnp.int32, (tok, tok), 0)
        < lax.broadcasted_iota(jnp.int32, (tok, tok), 1)
    ).astype(F32).astype(BF)
    expert = lax.broadcasted_iota(jnp.int32, (n_exp, tok), 0)
    ids = [ids_ref[k : k + 1, :] for k in range(2)]
    hot = [(i == expert).astype(F32) for i in ids]
    before = nn((hot[0] + hot[1]).astype(BF), up)
    slot_iota = lax.broadcasted_iota(jnp.int32, (total, tok), 0)
    lane = lax.broadcasted_iota(jnp.int32, (tok, tok), 1)
    place, sent, cols = [], [], []
    for k in range(2):
        slot = jnp.sum(before * hot[k], axis=0, keepdims=True)
        dest = ids[k].astype(F32) * cap + slot
        cols.append(jnp.broadcast_to(dest, (tok, tok)).T.astype(jnp.int32))
        place.append((slot_iota == dest.astype(jnp.int32)).astype(F32).astype(BF))
        weight = jnp.broadcast_to(w_ref[k : k + 1, :], (tok, tok)).T
        sent.append(
            jnp.concatenate(
                [(weight * og_ref[:, j : j + tok].astype(F32)).astype(BF) for j in range(0, ch, tok)], axis=1
            )
        )
    sx = nn(place[0] + place[1], x_ref[...]).astype(BF)
    sy = (nn(place[0], sent[0]) + nn(place[1], sent[1])).astype(BF)
    send_ref[:, :cap, :] = sx.reshape(n_exp, cap, ch)
    send_ref[:, cap:, :] = sy.reshape(n_exp, cap, ch)
    for j in range(total // tok):
        hit = (cols[0] == lane + j * tok) | (cols[1] == lane + j * tok)
        sel_ref[:, j * tok : (j + 1) * tok] = hit.astype(F32).astype(BF)


def mixed_kernel(b_ref, co_ref, mixed_ref):
    mixed_ref[...] = (b_ref[...].astype(F32) * co_ref[...].astype(F32)).astype(BF)


def load_kernel(gate_ref, up_ref, down_ref, w_ref, wd_ref, sems):
    width = wd_ref.shape[0]
    loads = [
        pltpu.make_async_copy(gate_ref, w_ref.at[pl.ds(0, width)], sems.at[0]),
        pltpu.make_async_copy(up_ref, w_ref.at[pl.ds(width, width)], sems.at[1]),
        pltpu.make_async_copy(down_ref, wd_ref, sems.at[2]),
    ]
    for load in loads:
        load.start()
    for load in loads:
        load.wait()


def expert_kernel(y_ref, c_ref, *refs):
    pieces, w_ref, wd_ref = refs[:16], refs[16], refs[17]
    theirs_ref, x_ref, dy_ref, hid_ref, dgu_ref, d_ref, gu_s, h_s = refs[18:]
    y, c = y_ref[0], c_ref[0]
    ch = pieces[0].shape[1]
    f = hid_ref.shape[0]
    for d in range(4):
        for other in range(2):
            o = channels(y, d, c if other == 0 else 1 - c, ch)
            x_ref[:, pl.ds(o, ch)] = pieces[4 * d + 2 * other][...]
            dy_ref[:, pl.ds(o, ch)] = pieces[4 * d + 2 * other + 1][...]
    gu_s[...] = nt(w_ref[...], x_ref[...])
    h_s[...] = nt(wd_ref[...], dy_ref[...])
    step = 32
    for r in range(0, f, step):
        g, u, dh = gu_s[r : r + step], gu_s[f + r : f + r + step], h_s[r : r + step]
        sig = jax.nn.sigmoid(g)
        act = g * sig
        hid_ref[r : r + step] = (act * u).astype(BF)
        dgu_ref[r : r + step] = (dh * u * (sig * (1.0 + g * (1.0 - sig)))).astype(BF)
        dgu_ref[f + r : f + r + step] = (dh * act).astype(BF)
    d_ref[...] = dgu_ref[...].T
    for d in range(4):
        o = channels(y, d, 1 - c, ch)
        theirs_ref[d] = nn(d_ref[...], w_ref[:, pl.ds(o, ch)]).astype(BF)


def channels(y, d, core, ch):
    return pl.multiple_of(ch * (2 * (y ^ d) + core), ch)


def own_half_kernel(y_ref, c_ref, d_ref, w_ref, mine_ref):
    y, c = y_ref[0], c_ref[0]
    ch = mine_ref.shape[2]
    for d in range(4):
        o = channels(y, d, c, ch)
        mine_ref[d] = nn(d_ref[...], w_ref[:, pl.ds(o, ch)]).astype(BF)


def pair_kernel(mine_ref, got_ref, keep_ref, *out_refs):
    half = keep_ref.shape[0] // 2
    keep_ref[...] = (mine_ref[0].astype(F32) + got_ref[0].astype(F32)).astype(BF)
    for d in range(1, 4):
        for k in range(2):
            rows = slice(k * half, (k + 1) * half)
            out_refs[2 * d - 2 + k][...] = (mine_ref[d, rows].astype(F32) + got_ref[d, rows].astype(F32)).astype(BF)


def halves_kernel(keep_ref, in1_ref, in3_ref, out1_ref, out3_ref, sum_ref):
    half = keep_ref.shape[0] // 2
    for at, one, three in ((0, in1_ref, out3_ref), (half, out1_ref, in3_ref)):
        total = keep_ref[at : at + half].astype(F32) + one[...].astype(F32) + three[...].astype(F32)
        sum_ref[at : at + half] = total.astype(BF)


def sum_kernel(*refs):
    total = refs[0][...].astype(F32)
    for ref in refs[1:-1]:
        total = total + ref[...].astype(F32)
    refs[-1][...] = total.astype(refs[-1].dtype)


def weights_kernel(x_ref, dy_ref, hid_ref, dgu_ref, gg_ref, gu_ref, gd_ref):
    f = hid_ref.shape[0]
    gg_ref[...] = nn(dgu_ref[:f], x_ref[...]).astype(BF)
    gu_ref[...] = nn(dgu_ref[f:], x_ref[...]).astype(BF)
    gd_ref[...] = nn(hid_ref[...], dy_ref[...]).astype(BF)


def combine_kernel(xi_ref, sel_ref, back_ref, og_ref, b_ref, dh_ref, one_ref, two_ref):
    dh = (og_ref[...].astype(F32) + nn(sel_ref[...], back_ref[...])).astype(BF)
    dh_ref[...] = dh
    tok = dh.shape[0]
    even = xi_ref[0] % 2 == 0
    for k, source in enumerate((dh_ref, b_ref)):
        first, last = source[0:1].astype(F32), source[tok - 1 :].astype(F32)
        one_ref[k : k + 1] = jnp.where(even, last, first).astype(BF)
        two_ref[k : k + 1] = jnp.where(even, first, last).astype(BF)


def stack_kernel(turned_ref, dh_ref, low_ref, high_ref, out_ref):
    tok, ch = turned_ref.shape
    out_ref[:tok] = turned_ref[...]
    out_ref[tok : 2 * tok] = dh_ref[...]
    row = lax.broadcasted_iota(jnp.int32, (16, ch), 0)
    low, high = low_ref[0:1].astype(F32), high_ref[0:1].astype(F32)
    out_ref[2 * tok :] = jnp.where(row == 0, low, jnp.where(row == 1, high, 0.0)).astype(BF)


def mixer_kernel(
    y_ref, c_ref, xi_ref, own_ref, part_ref, w_ref, b_ref, co_ref, bl_ref, bh_ref, t_ref, v_ref, g_ref,
    gb_ref, gc_ref, gv_ref,
):
    y, c = y_ref[0], c_ref[0]
    tok, ch = b_ref.shape
    size = own_ref.shape[0] // 4
    acc = jnp.zeros((size - tok, ch), F32)
    for d in range(4):
        for ref, core in ((own_ref, c), (part_ref, 1 - c)):
            acc = acc + nn(ref[d * size + tok : (d + 1) * size, :], w_ref[pl.ds(channels(y, d, core, ch), ch), :])
    gb_ref[...] = (acc[:tok] * co_ref[...].astype(F32)).astype(BF)
    dc = (acc[:tok] * b_ref[...].astype(F32)).astype(BF).astype(F32)
    one = (acc[tok : tok + 1] * bl_ref[1:2].astype(F32)).astype(BF).astype(F32)
    two = (acc[tok + 1 : tok + 2] * bh_ref[1:2].astype(F32)).astype(BF).astype(F32)
    even = xi_ref[0] % 2 == 0
    low, high = jnp.where(even, two, one), jnp.where(even, one, two)
    row = lax.broadcasted_iota(jnp.int32, dc.shape, 0)
    nxt = jnp.where(row == tok - 1, high, pltpu.roll(dc, tok - 1, 0))
    prv = jnp.where(row == 0, low, pltpu.roll(dc, 1, 0))
    du = t_ref[0:1, :] * nxt + t_ref[1:2, :] * dc + t_ref[2:3, :] * prv
    gc_ref[...] = (du * v_ref[...].astype(F32)).astype(BF)
    gv_ref[...] = (du * g_ref[...].astype(F32)).astype(BF)


def outer_kernel(y_ref, c_ref, z_ref, xi_ref, own_ref, part_ref, mix_ref, *refs):
    out_refs, (a_s, b_s, o_s) = refs[:4], refs[4:]
    y, c, z = y_ref[0], c_ref[0], z_ref[0]
    tok = mix_ref.shape[0] // 8
    size = own_ref.shape[0] // 4
    for d in range(4):
        for ref, core in ((own_ref, c), (part_ref, 1 - c)):
            a_s[pl.ds(channels(y, d, core, tok), tok), :] = ref[d * size : d * size + tok, :]
    for d, bits in enumerate((0, 4, 2, 6, 1, 5, 3, 7)):
        o = pl.multiple_of(tok * (z ^ bits), tok)
        b_s[pl.ds(o, tok), :] = mix_ref[d * tok : (d + 1) * tok, :]
    o_s[...] = tn(a_s[...], b_s[...])
    rows = out_refs[0].shape[0]
    for k, ref in enumerate(out_refs):
        ref[...] = o_s[pl.ds(pl.multiple_of(rows * (xi_ref[0] ^ k), rows), rows), :].astype(BF)


def over_tp(x):
    parts = [x] + [shift(x, "y", 4, k) for k in (1, 2, 3)]
    own = jnp.concatenate(parts, axis=0)
    return own, shift(own, "c", 2, 1)


def edges(one, two):
    n = lax.axis_size(SP)
    one = lax.ppermute(one, SP, [(i, i ^ 1) for i in range(n)])
    two = lax.ppermute(two, SP, [(i, i + 1 if i % 2 else i - 1) for i in range(1, n - 1)])
    return one, two


def widen(x, bit):
    return jnp.concatenate([x, lax.ppermute(x, "z", [(i, i ^ bit) for i in range(8)])], axis=0)


def local(
    out_grad, moe_input, route_weight, route_ids, gate_proj, up_proj, down_proj,
    out_proj, conv_out, gate_b, gate_c, value_v, conv_taps,
):
    tok, ch = out_grad.shape
    n_exp = lax.axis_size(SP)
    cap = 4 * tok // n_exp
    total = n_exp * cap
    yi = lax.axis_index("y").astype(jnp.int32).reshape(1)
    ci = lax.axis_index("c").astype(jnp.int32).reshape(1)
    zi = lax.axis_index("z").astype(jnp.int32).reshape(1)
    xi = lax.axis_index("x").astype(jnp.int32).reshape(1)
    yi, ci, zi, xi, moe_input = lax.optimization_barrier((yi, ci, zi, xi, moe_input))
    send, sel = call(
        dispatch_kernel,
        [(n_exp, 2 * cap, ch), (tok, total)],
        0,
        (moe_input, out_grad, route_weight.T, route_ids.T),
        hbm_args=(0, 1, 2, 3),
    )
    recv = lax.all_to_all(send, SP, 0, 0, tiled=True)
    recv, gate_b, conv_out, gate_proj, up_proj, down_proj = lax.optimization_barrier(
        (recv, gate_b, conv_out, gate_proj, up_proj, down_proj)
    )
    (mixed,) = call(mixed_kernel, [(tok, ch)], 0, (gate_b, conv_out), hbm_args=(0, 1))
    hx = recv[:, :cap].reshape(total, ch)
    hy = recv[:, cap:].reshape(total, ch)
    ax = shift(hx, "y", 4, 1)
    by = shift(hy, "y", 4, 3)
    ay = shift(hy, "y", 4, 1)
    bx = shift(hx, "y", 4, 3)
    mix = widen(mixed, 4)
    f, d = down_proj.shape[1:]
    w_pair, w_down = call(
        load_kernel,
        [(2 * f, d), (f, d)],
        0,
        (gate_proj[0].T, up_proj[0].T, down_proj[0]),
        scratch=[pltpu.SemaphoreType.DMA((3,))],
        any_args=(0, 1, 2),
    )
    bx, ay, w_pair, w_down = lax.optimization_barrier((bx, ay, w_pair, w_down))
    fx = shift(bx, "y", 4, 1)
    fy = shift(ay, "y", 4, 3)
    mix = widen(mix, 2)
    pieces = []
    for px, py in ((hx, hy), (ax, ay), (fx, fy), (bx, by)):
        pieces += [px, py, shift(px, "c", 2, 1), shift(py, "c", 2, 1)]
    mix = widen(mix, 1)
    theirs, xin, dyin, hidden, dgu, dgu_rows = call(
        expert_kernel,
        [(4, total, ch), (total, d), (total, d), (f, total), (2 * f, total), (total, 2 * f)],
        2,
        (yi, ci, *pieces, w_pair, w_down),
        scratch=[pltpu.VMEM((2 * f, total), F32), pltpu.VMEM((f, total), F32)],
        flops=8 * total * d * f,
        limit=24,
    )
    got = shift(theirs, "c", 2, 1)
    (mine,) = call(own_half_kernel, [(4, total, ch)], 2, (yi, ci, dgu_rows, w_pair), flops=2 * total * d * f)
    half = total // 2
    keep, lo1, hi1, lo2, hi2, lo3, hi3 = call(pair_kernel, [(total, ch)] + [(half, ch)] * 6, 0, (mine, got))
    via1 = shift(lo2, "y", 4, 1)
    via3 = shift(hi2, "y", 4, 3)
    in1 = shift(lo1, "y", 4, 1)
    in3 = shift(hi3, "y", 4, 3)
    (lo3,) = call(sum_kernel, [(half, ch)], 0, (lo3, via1))
    out3 = shift(lo3, "y", 4, 3)
    (hi1,) = call(sum_kernel, [(half, ch)], 0, (hi1, via3))
    out1 = shift(hi1, "y", 4, 1)
    parts = (in1, in3, out1, out3)
    gate_t, up_t, grad_down = call(
        weights_kernel,
        [(f, d)] * 3,
        0,
        (xin, dyin, hidden, dgu),
        flops=6 * total * d * f,
        hbm_outs=(0, 1, 2),
        limit=24,
    )
    parts, mix, gate_t, up_t, grad_down = lax.optimization_barrier((parts, mix, gate_t, up_t, grad_down))
    (summed,) = call(halves_kernel, [(total, ch)], 0, (keep, *parts))
    back = lax.all_to_all(summed.reshape(n_exp, cap, ch), SP, 0, 0, tiled=True)
    dh, one, two = call(
        combine_kernel, [(tok, ch), (2, ch), (2, ch)], 1, (xi, sel, back.reshape(total, ch), out_grad, gate_b)
    )
    swap = [(z * 8 + y * 2 + c, (y * 2 + c) * 8 + z) for z in range(8) for y in range(4) for c in range(2)]
    turned = lax.ppermute(dh, ("z", "y", "c"), swap)
    one, two = edges(one, two)
    (stack,) = call(stack_kernel, [(2 * tok + 16, ch)], 0, (turned, dh, one, two))
    own, part = over_tp(stack)
    terms = call(
        outer_kernel,
        [(ch // 4, ch)] * 4,
        4,
        (yi, ci, zi, xi, own, part, mix),
        scratch=[pltpu.VMEM((8 * tok, ch), BF)] * 2 + [pltpu.VMEM((ch, ch), F32)],
        flops=16 * tok * ch * ch,
    )
    came = [shift(terms[k], "x", 4, k) for k in (1, 3, 2)]
    grad_b, grad_c, grad_v = call(
        mixer_kernel,
        [(tok, ch)] * 3,
        3,
        (yi, ci, xi, own, part, out_proj, gate_b, conv_out, one, two, conv_taps, value_v, gate_c),
        flops=2 * tok * d * ch,
        hbm_outs=(0, 1, 2),
    )
    (grad_out,) = call(sum_kernel, [(ch // 4, ch)], 0, (terms[0], *came), hbm_outs=(0,), kind=F32)
    return (gate_t.T[None], up_t.T[None], grad_down[None], grad_out, grad_b, grad_c, grad_v)


def solution(mesh):
    split = Mesh(mesh.devices.reshape(8, 4, 4, 2), ("z", "x", "y", "c"))
    return jax.shard_map(
        local,
        mesh=split,
        in_specs=(
            P(SP, TP), P(SP, TP), P(SP, None), P(SP, None), P(SP, None, TP), P(SP, None, TP),
            P(SP, TP, None), P(None, TP), P(SP, TP), P(SP, TP), P(SP, TP), P(SP, TP), P(None, TP),
        ),
        out_specs=(
            P(SP, None, TP), P(SP, None, TP), P(SP, TP, None), P(SP, TP), P(SP, TP), P(SP, TP), P(SP, TP),
        ),
        check_vma=False,
    )
```

```python
import jax
import jax.numpy as jnp
from jax import lax
from jax.experimental import pallas as pl
from jax.experimental.pallas import tpu as pltpu
from jax.sharding import Mesh
from jax.sharding import PartitionSpec as P

SP = ("z", "x")
TP = ("y", "c")
BF = jnp.bfloat16
F32 = jnp.float32

VMEM = pl.BlockSpec(memory_space=pltpu.VMEM)
SMEM = pl.BlockSpec(memory_space=pltpu.SMEM)
ANY = pl.BlockSpec(memory_space=pltpu.HBM)


def call(body, outs, n_smem, args, scratch=(), flops=0, hbm_outs=(), limit=8, hbm_args=(), any_args=(), kind=BF):
    args = [
        a if i < n_smem else pltpu.with_memory_space_constraint(a, pltpu.HBM if i in hbm_args or i in any_args else pltpu.VMEM)
        for i, a in enumerate(args)
    ]
    outs = [
        jax.ShapeDtypeStruct(shape, kind) if i in hbm_outs else pltpu.VMEM(shape, BF)
        for i, shape in enumerate(outs)
    ]
    return pl.pallas_call(
        body,
        out_shape=outs,
        in_specs=[SMEM if i < n_smem else ANY if i in any_args else VMEM for i in range(len(args))],
        out_specs=[VMEM] * len(outs),
        scratch_shapes=list(scratch),
        cost_estimate=pl.CostEstimate(flops=flops, bytes_accessed=0, transcendentals=0),
        compiler_params=pltpu.CompilerParams(vmem_limit_bytes=limit << 20),
    )(*args)


def nt(a, b):
    return lax.dot_general(a, b, (((1,), (1,)), ((), ())), preferred_element_type=F32)


def tn(a, b):
    return lax.dot_general(a, b, (((0,), (0,)), ((), ())), preferred_element_type=F32)


def nn(a, b):
    return jnp.dot(a, b, preferred_element_type=F32)


def shift(x, axis, n, k):
    return lax.ppermute(x, axis, [(i, i ^ k) for i in range(n)])


def dispatch_kernel(x_ref, og_ref, w_ref, ids_ref, send_ref, sel_ref):
    tok, ch = x_ref.shape
    n_exp, cap2, _ = send_ref.shape
    cap = cap2 // 2
    total = n_exp * cap
    up = (
        lax.broadcasted_iota(jnp.int32, (tok, tok), 0)
        < lax.broadcasted_iota(jnp.int32, (tok, tok), 1)
    ).astype(F32).astype(BF)
    expert = lax.broadcasted_iota(jnp.int32, (n_exp, tok), 0)
    ids = [ids_ref[k : k + 1, :] for k in range(2)]
    hot = [(i == expert).astype(F32) for i in ids]
    before = nn((hot[0] + hot[1]).astype(BF), up)
    slot_iota = lax.broadcasted_iota(jnp.int32, (total, tok), 0)
    lane = lax.broadcasted_iota(jnp.int32, (tok, tok), 1)
    place, sent, cols = [], [], []
    for k in range(2):
        slot = jnp.sum(before * hot[k], axis=0, keepdims=True)
        dest = ids[k].astype(F32) * cap + slot
        cols.append(jnp.broadcast_to(dest, (tok, tok)).T.astype(jnp.int32))
        place.append((slot_iota == dest.astype(jnp.int32)).astype(F32).astype(BF))
        weight = jnp.broadcast_to(w_ref[k : k + 1, :], (tok, tok)).T
        sent.append(
            jnp.concatenate(
                [(weight * og_ref[:, j : j + tok].astype(F32)).astype(BF) for j in range(0, ch, tok)], axis=1
            )
        )
    sx = nn(place[0] + place[1], x_ref[...]).astype(BF)
    sy = (nn(place[0], sent[0]) + nn(place[1], sent[1])).astype(BF)
    send_ref[:, :cap, :] = sx.reshape(n_exp, cap, ch)
    send_ref[:, cap:, :] = sy.reshape(n_exp, cap, ch)
    for j in range(total // tok):
        hit = (cols[0] == lane + j * tok) | (cols[1] == lane + j * tok)
        sel_ref[:, j * tok : (j + 1) * tok] = hit.astype(F32).astype(BF)


def mixed_kernel(b_ref, co_ref, mixed_ref):
    mixed_ref[...] = (b_ref[...].astype(F32) * co_ref[...].astype(F32)).astype(BF)


def load_kernel(gate_ref, up_ref, down_ref, w_ref, wd_ref, sems):
    width = wd_ref.shape[0]
    loads = [
        pltpu.make_async_copy(gate_ref, w_ref.at[pl.ds(0, width)], sems.at[0]),
        pltpu.make_async_copy(up_ref, w_ref.at[pl.ds(width, width)], sems.at[1]),
        pltpu.make_async_copy(down_ref, wd_ref, sems.at[2]),
    ]
    for load in loads:
        load.start()
    for load in loads:
        load.wait()


def expert_kernel(y_ref, c_ref, *refs):
    pieces, w_ref, wd_ref = refs[:16], refs[16], refs[17]
    theirs_ref, x_ref, dy_ref, hid_ref, dgu_ref, d_ref, gu_s, h_s = refs[18:]
    y, c = y_ref[0], c_ref[0]
    ch = pieces[0].shape[1]
    f = hid_ref.shape[0]
    for d in range(4):
        for other in range(2):
            o = channels(y, d, c if other == 0 else 1 - c, ch)
            x_ref[:, pl.ds(o, ch)] = pieces[4 * d + 2 * other][...]
            dy_ref[:, pl.ds(o, ch)] = pieces[4 * d + 2 * other + 1][...]
    gu_s[...] = nt(w_ref[...], x_ref[...])
    h_s[...] = nt(wd_ref[...], dy_ref[...])
    step = 32
    for r in range(0, f, step):
        g, u, dh = gu_s[r : r + step], gu_s[f + r : f + r + step], h_s[r : r + step]
        sig = jax.nn.sigmoid(g)
        act = g * sig
        hid_ref[r : r + step] = (act * u).astype(BF)
        dgu_ref[r : r + step] = (dh * u * (sig * (1.0 + g * (1.0 - sig)))).astype(BF)
        dgu_ref[f + r : f + r + step] = (dh * act).astype(BF)
    d_ref[...] = dgu_ref[...].T
    for d in range(4):
        o = channels(y, d, 1 - c, ch)
        theirs_ref[d] = nn(d_ref[...], w_ref[:, pl.ds(o, ch)]).astype(BF)


def channels(y, d, core, ch):
    return pl.multiple_of(ch * (2 * (y ^ d) + core), ch)


def own_half_kernel(y_ref, c_ref, d_ref, w_ref, mine_ref):
    y, c = y_ref[0], c_ref[0]
    ch = mine_ref.shape[2]
    for d in range(4):
        o = channels(y, d, c, ch)
        mine_ref[d] = nn(d_ref[...], w_ref[:, pl.ds(o, ch)]).astype(BF)


def pair_kernel(mine_ref, got_ref, keep_ref, *out_refs):
    half = keep_ref.shape[0] // 2
    keep_ref[...] = (mine_ref[0].astype(F32) + got_ref[0].astype(F32)).astype(BF)
    for d in range(1, 4):
        for k in range(2):
            rows = slice(k * half, (k + 1) * half)
            out_refs[2 * d - 2 + k][...] = (mine_ref[d, rows].astype(F32) + got_ref[d, rows].astype(F32)).astype(BF)


def halves_kernel(keep_ref, in1_ref, in3_ref, out1_ref, out3_ref, sum_ref):
    half = keep_ref.shape[0] // 2
    for at, one, three in ((0, in1_ref, out3_ref), (half, out1_ref, in3_ref)):
        total = keep_ref[at : at + half].astype(F32) + one[...].astype(F32) + three[...].astype(F32)
        sum_ref[at : at + half] = total.astype(BF)


def sum_kernel(*refs):
    total = refs[0][...].astype(F32)
    for ref in refs[1:-1]:
        total = total + ref[...].astype(F32)
    refs[-1][...] = total.astype(refs[-1].dtype)


def weights_kernel(x_ref, dgu_ref, gg_ref, gu_ref):
    f = gg_ref.shape[0]
    gg_ref[...] = nn(dgu_ref[:f], x_ref[...]).astype(BF)
    gu_ref[...] = nn(dgu_ref[f:], x_ref[...]).astype(BF)


def down_kernel(hid_ref, dy_ref, gd_ref):
    gd_ref[...] = nn(hid_ref[...], dy_ref[...]).astype(BF)


def combine_kernel(xi_ref, sel_ref, back_ref, og_ref, b_ref, dh_ref, one_ref, two_ref):
    dh = (og_ref[...].astype(F32) + nn(sel_ref[...], back_ref[...])).astype(BF)
    dh_ref[...] = dh
    tok = dh.shape[0]
    even = xi_ref[0] % 2 == 0
    for k, source in enumerate((dh_ref, b_ref)):
        first, last = source[0:1].astype(F32), source[tok - 1 :].astype(F32)
        one_ref[k : k + 1] = jnp.where(even, last, first).astype(BF)
        two_ref[k : k + 1] = jnp.where(even, first, last).astype(BF)


def stack_kernel(turned_ref, dh_ref, low_ref, high_ref, out_ref):
    tok, ch = turned_ref.shape
    out_ref[:tok] = turned_ref[...]
    out_ref[tok : 2 * tok] = dh_ref[...]
    row = lax.broadcasted_iota(jnp.int32, (16, ch), 0)
    low, high = low_ref[0:1].astype(F32), high_ref[0:1].astype(F32)
    out_ref[2 * tok :] = jnp.where(row == 0, low, jnp.where(row == 1, high, 0.0)).astype(BF)


def mixer_kernel(
    y_ref, c_ref, xi_ref, own_ref, part_ref, w_ref, b_ref, co_ref, bl_ref, bh_ref, t_ref, v_ref, g_ref,
    gb_ref, gc_ref, gv_ref,
):
    y, c = y_ref[0], c_ref[0]
    tok, ch = b_ref.shape
    size = own_ref.shape[0] // 4
    acc = jnp.zeros((size - tok, ch), F32)
    for d in range(4):
        for ref, core in ((own_ref, c), (part_ref, 1 - c)):
            acc = acc + nn(ref[d * size + tok : (d + 1) * size, :], w_ref[pl.ds(channels(y, d, core, ch), ch), :])
    gb_ref[...] = (acc[:tok] * co_ref[...].astype(F32)).astype(BF)
    dc = (acc[:tok] * b_ref[...].astype(F32)).astype(BF).astype(F32)
    one = (acc[tok : tok + 1] * bl_ref[1:2].astype(F32)).astype(BF).astype(F32)
    two = (acc[tok + 1 : tok + 2] * bh_ref[1:2].astype(F32)).astype(BF).astype(F32)
    even = xi_ref[0] % 2 == 0
    low, high = jnp.where(even, two, one), jnp.where(even, one, two)
    row = lax.broadcasted_iota(jnp.int32, dc.shape, 0)
    nxt = jnp.where(row == tok - 1, high, pltpu.roll(dc, tok - 1, 0))
    prv = jnp.where(row == 0, low, pltpu.roll(dc, 1, 0))
    du = t_ref[0:1, :] * nxt + t_ref[1:2, :] * dc + t_ref[2:3, :] * prv
    gc_ref[...] = (du * v_ref[...].astype(F32)).astype(BF)
    gv_ref[...] = (du * g_ref[...].astype(F32)).astype(BF)


def outer_kernel(y_ref, c_ref, z_ref, xi_ref, own_ref, part_ref, mix_ref, *refs):
    out_refs, (a_s, b_s, o_s) = refs[:4], refs[4:]
    y, c, z = y_ref[0], c_ref[0], z_ref[0]
    tok = mix_ref.shape[0] // 8
    size = own_ref.shape[0] // 4
    for d in range(4):
        for ref, core in ((own_ref, c), (part_ref, 1 - c)):
            a_s[pl.ds(channels(y, d, core, tok), tok), :] = ref[d * size : d * size + tok, :]
    for d, bits in enumerate((0, 4, 2, 6, 1, 5, 3, 7)):
        o = pl.multiple_of(tok * (z ^ bits), tok)
        b_s[pl.ds(o, tok), :] = mix_ref[d * tok : (d + 1) * tok, :]
    o_s[...] = tn(a_s[...], b_s[...])
    rows = out_refs[0].shape[0]
    for k, ref in enumerate(out_refs):
        ref[...] = o_s[pl.ds(pl.multiple_of(rows * (xi_ref[0] ^ k), rows), rows), :].astype(BF)


def over_tp(x):
    parts = [x] + [shift(x, "y", 4, k) for k in (1, 2, 3)]
    own = jnp.concatenate(parts, axis=0)
    return own, shift(own, "c", 2, 1)


def edges(one, two):
    n = lax.axis_size(SP)
    one = lax.ppermute(one, SP, [(i, i ^ 1) for i in range(n)])
    two = lax.ppermute(two, SP, [(i, i + 1 if i % 2 else i - 1) for i in range(1, n - 1)])
    return one, two


def widen(x, bit):
    return jnp.concatenate([x, lax.ppermute(x, "z", [(i, i ^ bit) for i in range(8)])], axis=0)


def local(
    out_grad, moe_input, route_weight, route_ids, gate_proj, up_proj, down_proj,
    out_proj, conv_out, gate_b, gate_c, value_v, conv_taps,
):
    tok, ch = out_grad.shape
    n_exp = lax.axis_size(SP)
    cap = 4 * tok // n_exp
    total = n_exp * cap
    yi = lax.axis_index("y").astype(jnp.int32).reshape(1)
    ci = lax.axis_index("c").astype(jnp.int32).reshape(1)
    zi = lax.axis_index("z").astype(jnp.int32).reshape(1)
    xi = lax.axis_index("x").astype(jnp.int32).reshape(1)
    yi, ci, zi, xi, moe_input = lax.optimization_barrier((yi, ci, zi, xi, moe_input))
    send, sel = call(
        dispatch_kernel,
        [(n_exp, 2 * cap, ch), (tok, total)],
        0,
        (moe_input, out_grad, route_weight.T, route_ids.T),
        hbm_args=(0, 1, 2, 3),
    )
    recv = lax.all_to_all(send, SP, 0, 0, tiled=True)
    recv, gate_b, conv_out, gate_proj, up_proj, down_proj = lax.optimization_barrier(
        (recv, gate_b, conv_out, gate_proj, up_proj, down_proj)
    )
    (mixed,) = call(mixed_kernel, [(tok, ch)], 0, (gate_b, conv_out), hbm_args=(0, 1))
    hx = recv[:, :cap].reshape(total, ch)
    hy = recv[:, cap:].reshape(total, ch)
    ax = shift(hx, "y", 4, 1)
    by = shift(hy, "y", 4, 3)
    ay = shift(hy, "y", 4, 1)
    bx = shift(hx, "y", 4, 3)
    mix = widen(mixed, 4)
    f, d = down_proj.shape[1:]
    w_pair, w_down = call(
        load_kernel,
        [(2 * f, d), (f, d)],
        0,
        (gate_proj[0].T, up_proj[0].T, down_proj[0]),
        scratch=[pltpu.SemaphoreType.DMA((3,))],
        any_args=(0, 1, 2),
    )
    bx, ay, w_pair, w_down = lax.optimization_barrier((bx, ay, w_pair, w_down))
    fx = shift(bx, "y", 4, 1)
    fy = shift(ay, "y", 4, 3)
    mix = widen(mix, 2)
    pieces = []
    for px, py in ((hx, hy), (ax, ay), (fx, fy), (bx, by)):
        pieces += [px, py, shift(px, "c", 2, 1), shift(py, "c", 2, 1)]
    mix = widen(mix, 1)
    theirs, xin, dyin, hidden, dgu, dgu_rows = call(
        expert_kernel,
        [(4, total, ch), (total, d), (total, d), (f, total), (2 * f, total), (total, 2 * f)],
        2,
        (yi, ci, *pieces, w_pair, w_down),
        scratch=[pltpu.VMEM((2 * f, total), F32), pltpu.VMEM((f, total), F32)],
        flops=8 * total * d * f,
        limit=24,
    )
    got = shift(theirs, "c", 2, 1)
    (mine,) = call(own_half_kernel, [(4, total, ch)], 2, (yi, ci, dgu_rows, w_pair), flops=2 * total * d * f)
    half = total // 2
    keep, lo1, hi1, lo2, hi2, lo3, hi3 = call(pair_kernel, [(total, ch)] + [(half, ch)] * 6, 0, (mine, got))
    via1 = shift(lo2, "y", 4, 1)
    via3 = shift(hi2, "y", 4, 3)
    in1 = shift(lo1, "y", 4, 1)
    in3 = shift(hi3, "y", 4, 3)
    (lo3,) = call(sum_kernel, [(half, ch)], 0, (lo3, via1))
    out3 = shift(lo3, "y", 4, 3)
    (hi1,) = call(sum_kernel, [(half, ch)], 0, (hi1, via3))
    out1 = shift(hi1, "y", 4, 1)
    parts = (in1, in3, out1, out3)
    gate_t, up_t = call(weights_kernel, [(f, d)] * 2, 0, (xin, dgu), flops=4 * total * d * f, hbm_outs=(0, 1), limit=24)
    parts, mix, gate_t, up_t = lax.optimization_barrier((parts, mix, gate_t, up_t))
    (summed,) = call(halves_kernel, [(total, ch)], 0, (keep, *parts))
    back = lax.all_to_all(summed.reshape(n_exp, cap, ch), SP, 0, 0, tiled=True)
    dh, one, two = call(
        combine_kernel, [(tok, ch), (2, ch), (2, ch)], 1, (xi, sel, back.reshape(total, ch), out_grad, gate_b)
    )
    swap = [(z * 8 + y * 2 + c, (y * 2 + c) * 8 + z) for z in range(8) for y in range(4) for c in range(2)]
    turned = lax.ppermute(dh, ("z", "y", "c"), swap)
    (grad_down,) = call(
        down_kernel, [(f, d)], 0, (hidden, dyin), flops=2 * total * d * f, hbm_outs=(0,), limit=12
    )
    one, two = edges(one, two)
    (stack,) = call(stack_kernel, [(2 * tok + 16, ch)], 0, (turned, dh, one, two))
    own, part = over_tp(stack)
    terms = call(
        outer_kernel,
        [(ch // 4, ch)] * 4,
        4,
        (yi, ci, zi, xi, own, part, mix),
        scratch=[pltpu.VMEM((8 * tok, ch), BF)] * 2 + [pltpu.VMEM((ch, ch), F32)],
        flops=16 * tok * ch * ch,
    )
    came = [shift(terms[k], "x", 4, k) for k in (1, 3, 2)]
    grad_b, grad_c, grad_v = call(
        mixer_kernel,
        [(tok, ch)] * 3,
        3,
        (yi, ci, xi, own, part, out_proj, gate_b, conv_out, one, two, conv_taps, value_v, gate_c),
        flops=2 * tok * d * ch,
        hbm_outs=(0, 1, 2),
    )
    (grad_out,) = call(sum_kernel, [(ch // 4, ch)], 0, (terms[0], *came), hbm_outs=(0,), kind=F32)
    return (gate_t.T[None], up_t.T[None], grad_down[None], grad_out, grad_b, grad_c, grad_v)


def solution(mesh):
    split = Mesh(mesh.devices.reshape(8, 4, 4, 2), ("z", "x", "y", "c"))
    return jax.shard_map(
        local,
        mesh=split,
        in_specs=(
            P(SP, TP), P(SP, TP), P(SP, None), P(SP, None), P(SP, None, TP), P(SP, None, TP),
            P(SP, TP, None), P(None, TP), P(SP, TP), P(SP, TP), P(SP, TP), P(SP, TP), P(None, TP),
        ),
        out_specs=(
            P(SP, None, TP), P(SP, None, TP), P(SP, TP, None), P(SP, TP), P(SP, TP), P(SP, TP), P(SP, TP),
        ),
        check_vma=False,
    )
```
